32 devices in a mesh: kv: 8 (over z, x), tp: 4 (over y, core).
Axes of the slice: x: 2, y: 2, z: 4, core: 2. Of those that a mesh axis runs over, the one named last changes fastest.
Arguments:
- inputs: bfloat16 [2048, 2048], P('kv', 'tp'), may hold values from -6 to 6
- queries: bfloat16 [2048, 2048], P('kv', 'tp'), may hold values from -8 to 8
- key_vectors: bfloat16 [2048, 512], P('kv', 'tp'), may hold values from -8 to 8
- value_rows_by_head: bfloat16 [2048, 512], P('kv', 'tp'), may hold values from -6 to 6
- out_grad: bfloat16 [2048, 2048], P('kv', 'tp'), may hold values from -6 to 6
- chosen: int32 [16, 16], replicated, may hold values from 0 to 31, as said below
Outputs:
- query_grad: bfloat16 [2048, 2048], P('kv', 'tp')
- key_grad: bfloat16 [2048, 512], P('kv', 'tp')
- value_grad: bfloat16 [2048, 512], P('kv', 'tp')
- weight_grad: float32 [2048, 2048], P('kv', 'tp')
The draws below stay inside these ranges and needn't reach their ends.
Inputs may be any that keep to these rules, and one draw needn't show every extreme that they name: `chosen`: row r holds 16 distinct key-block numbers, among them every key block that intersects query block r. The rows of one device (aligned runs of 2 rows) name at most 2 distinct key blocks that lie on any one other device (aligned runs of 4 key blocks), and exactly 2 at some other device for some devices.
All inputs are finite; a program needn't handle non-finite values.
Results may differ from the reference program's by a relative error of at most 0.015.
The reference program's roundings to bfloat16 on the way (of `probs_half` and `score_grad`) count: a program that leaves them out, or rounds other values in their place, can miss the bound.
Values may be sent and summed in bfloat16 or wider, within the bound.
A program may use at most 128 MiB of HBM per device.

```python
import jax
import jax.numpy as jnp
from jax import lax

D = 2048
QUERY_HEADS = 32
KEY_VALUE_HEADS = 8
HEAD_SIZE = 64
QB = 128
KB = 64
NSEL = 16
TOK_DEV = 256
SEQUENCE_TOKENS = 2048


def draw_queries(key, part):
    final_result = jnp.clip(jax.random.normal(jax.random.fold_in(key, 1), (SEQUENCE_TOKENS, QUERY_HEADS * HEAD_SIZE), jnp.float32), -6.0, 6.0)
    return final_result.astype(jnp.bfloat16)


def draw_key_vectors(key, part):
    final_result = jnp.clip(jax.random.normal(jax.random.fold_in(key, 2), (SEQUENCE_TOKENS, KEY_VALUE_HEADS * HEAD_SIZE), jnp.float32), -6.0, 6.0)
    return final_result.astype(jnp.bfloat16)


def draw_chosen(key, part):
    q_count = SEQUENCE_TOKENS // QB
    k_count = SEQUENCE_TOKENS // KB
    ratio = QB // KB
    owner_blocks = TOK_DEV // KB
    local_blocks = TOK_DEV // QB
    n_dev = SEQUENCE_TOKENS // TOK_DEV
    q_index = jnp.arange(q_count, dtype=jnp.int32)[:, None]
    k_index = jnp.arange(k_count, dtype=jnp.int32)[None, :]
    dev_grid = jnp.arange(n_dev, dtype=jnp.int32)[:, None]
    own_grid = jnp.arange(n_dev, dtype=jnp.int32)[None, :]
    random_phase = jax.random.randint(jax.random.fold_in(key, 7), (n_dev, n_dev), 0, ratio)
    phase = jnp.where(own_grid == (dev_grid - 1) % n_dev, ratio - 1, jnp.where(own_grid == (dev_grid - n_dev // 2) % n_dev, 0, random_phase))
    query_dev = q_index // local_blocks
    key_owner = k_index // owner_blocks
    key_offset = k_index % owner_blocks
    permitted = (key_owner == query_dev) | (key_offset % ratio == phase[query_dev, key_owner])
    own_block = k_index // ratio == q_index
    forced = (k_index == q_index * ratio - 1) | (k_index == q_index * ratio - k_count // 2)
    causal = k_index < q_index * ratio
    tier = jnp.where(own_block, 3, jnp.where(forced, 2, jnp.where(causal, 1, 0)))
    tier = jnp.where(permitted, tier, -1)
    popular = jax.random.randint(jax.random.fold_in(key, 5), (k_count,), 0, 2) * 7
    row_keys = jax.random.split(jax.random.fold_in(key, 6), q_count)
    noise = jax.vmap(lambda one_key: jax.random.permutation(one_key, k_count))(row_keys)
    ranking = tier * (k_count * 8) + popular[None, :] * k_count + noise
    _, picked = lax.top_k(ranking, NSEL)
    return picked.astype(jnp.int32)


def levels(rng, dims, shards, least, largest):
    loudness = 1.0
    for dim, parts in shards:
        draws = jax.random.uniform(jax.random.fold_in(jax.random.fold_in(rng, 6), dim), (parts,), jnp.float32, least / len(shards), largest / len(shards))
        loudness = loudness * jnp.repeat(jnp.exp(draws), dims[dim] // parts).reshape((-1,) + (1,) * (len(dims) - 1 - dim))
    return loudness


def centred(stream_key, dims, deviation, limit, shards=(), kind=jnp.bfloat16):
    level = levels(stream_key, dims, shards, -0.22, 0.18) if shards else 1.0
    entries = jax.random.normal(stream_key, dims, jnp.float32) * deviation * level
    return jnp.minimum(jnp.maximum(entries, -limit), limit).astype(kind)


def setup_inputs(seed: int = 0) -> dict:
    streams_of = jax.random.split(jax.random.key(seed), 7)
    inputs = centred(streams_of[0], (SEQUENCE_TOKENS, D), 1.0, 6.0, ((0, 8), (1, 4)))
    queries = draw_queries(jax.random.fold_in(streams_of[6], 71), 0)
    key_vectors = draw_key_vectors(jax.random.fold_in(streams_of[6], 71), 0)
    value_rows_by_head = centred(streams_of[3], (SEQUENCE_TOKENS, KEY_VALUE_HEADS * HEAD_SIZE), 1.0, 6.0, ((0, 8), (1, 4)))
    out_grad = centred(streams_of[4], (SEQUENCE_TOKENS, QUERY_HEADS * HEAD_SIZE), 1.0, 6.0, ((0, 8), (1, 4)))
    chosen = draw_chosen(jax.random.fold_in(streams_of[6], 71), 0)
    return dict(inputs=inputs, queries=queries, key_vectors=key_vectors, value_rows_by_head=value_rows_by_head, out_grad=out_grad, chosen=chosen)


def round_trip(values_in):
    halved = lax.optimization_barrier(values_in.astype(jnp.bfloat16))
    return halved.astype(jnp.float32)


def reference(inputs, queries, key_vectors, value_rows_by_head, out_grad, chosen):
    total = queries.shape[0]
    q_heads = queries.shape[1] // HEAD_SIZE
    kv_heads = key_vectors.shape[1] // HEAD_SIZE
    group_size = q_heads // kv_heads
    score_scale = HEAD_SIZE ** -0.5
    offsets = jnp.arange(KB, dtype=jnp.int32)

    def step(state_pair, q_blk):
        acc_k, acc_v = state_pair
        first = q_blk * QB
        q_block = lax.dynamic_slice_in_dim(queries, first, QB, 0).astype(jnp.float32).reshape(QB, kv_heads, group_size, HEAD_SIZE)
        g_block = lax.dynamic_slice_in_dim(out_grad, first, QB, 0).astype(jnp.float32).reshape(QB, kv_heads, group_size, HEAD_SIZE)
        key_rows = (chosen[q_blk][:, None] * KB + offsets[None, :]).reshape(-1).astype(jnp.int32)
        key_sel = key_vectors[key_rows].astype(jnp.float32).reshape(-1, kv_heads, HEAD_SIZE)
        val_sel = value_rows_by_head[key_rows].astype(jnp.float32).reshape(-1, kv_heads, HEAD_SIZE)
        positions = first + jnp.arange(QB, dtype=jnp.int32)
        allowed = key_rows[None, :] <= positions[:, None]
        scores = jnp.einsum('tkgd,skd->kgts', q_block, key_sel) * score_scale
        scores = jnp.where(allowed, scores, -1e30)
        row_max = jnp.max(scores, axis=-1, keepdims=True)
        log_sum = row_max + jnp.log(jnp.sum(jnp.exp(scores - row_max), axis=-1, keepdims=True))
        probs = jnp.exp(scores - log_sum)
        probs_half = round_trip(probs)
        attended = jnp.einsum('kgts,skd->tkgd', probs_half, val_sel)
        row_dot = jnp.einsum('tkgd,tkgd->kgt', g_block, attended)
        prob_grad = jnp.einsum('tkgd,skd->kgts', g_block, val_sel)
        score_grad = round_trip(probs * (prob_grad - row_dot[..., None]))
        d_query = jnp.einsum('kgts,skd->tkgd', score_grad, key_sel) * score_scale
        d_key = jnp.einsum('kgts,tkgd->skd', score_grad, q_block) * score_scale
        d_value = jnp.einsum('kgts,tkgd->skd', probs_half, g_block)
        acc_k = acc_k.at[key_rows].add(d_key.reshape(-1, kv_heads * HEAD_SIZE))
        acc_v = acc_v.at[key_rows].add(d_value.reshape(-1, kv_heads * HEAD_SIZE))
        return (acc_k, acc_v), d_query.reshape(QB, q_heads * HEAD_SIZE)

    zeros = jnp.zeros((total, kv_heads * HEAD_SIZE), jnp.float32)
    (acc_k, acc_v), query_blocks = lax.scan(step, (zeros, zeros), jnp.arange(total // QB, dtype=jnp.int32))
    query_grad = query_blocks.reshape(total, q_heads * HEAD_SIZE).astype(jnp.bfloat16)
    weight_grad = jnp.dot(inputs.T, query_grad, preferred_element_type=jnp.float32)
    return query_grad, acc_k.astype(jnp.bfloat16), acc_v.astype(jnp.bfloat16), weight_grad
```

```python
import functools

import jax
import jax.numpy as jnp
from jax import lax
from jax.experimental import pallas as pl
from jax.experimental.pallas import tpu as pltpu
from jax.sharding import PartitionSpec as P

HEAD_SIZE = 64
QB = 128
KB = 64
NEG = -1e30
BF16 = jnp.bfloat16
F32 = jnp.float32
MESH = pl.DeviceIdType.MESH


def dot_nt(x, y):
    return lax.dot_general(x, y, (((1,), (1,)), ((), ())), preferred_element_type=F32)


def dot_nn(x, y):
    return lax.dot_general(x, y, (((1,), (0,)), ((), ())), preferred_element_type=F32)


def dot_tn(x, y):
    return lax.dot_general(x, y, (((0,), (0,)), ((), ())), preferred_element_type=F32)


def kernel(
    n, tp, a, b,
    chosen_ref, x_ref, q_ref, k_ref, v_ref, g_ref,
    dq_ref, dk_ref, dv_ref, w_ref,
    ch_v, sel_v, sel_s, x_in, xst, q_in, g_in, k_in, v_in, qz, gz, kvown, kvst, kvbuf, xbuf,
    e_buf, dp_buf, mj_buf, dqt, gst, grecv, own_acc, qall, wst, wrecv, w_own,
    ld, kv_send, kv_recv, x_send, x_recv, f_send, g_send, g_recv, q_send, q_recv,
    w_send, w_recv,
):
    me = lax.axis_index("kv")
    t = lax.axis_index("tp")
    alpha = lax.rem(me, a)
    beta = lax.div(me, a)
    parity = lax.rem(t, 2)
    partner = t + 1 - 2 * parity
    rows, cols = k_in.shape
    heads = cols // HEAD_SIZE
    group = q_in.shape[1] // cols
    local = rows // QB
    owner = rows // KB
    chunk = local * KB
    wide = group * rows
    width = xst.shape[2]
    n_chunk = xst.shape[0]
    gcols = group * HEAD_SIZE
    scale = HEAD_SIZE ** (-0.5)
    single_at = rows
    pair_at = rows + chunk

    def remote(src, dst, send, recv, kv, tpi):
        return pltpu.make_async_remote_copy(
            src_ref=src, dst_ref=dst, send_sem=send, recv_sem=recv,
            device_id=(kv, tpi), device_id_type=MESH,
        )

    barrier = pltpu.get_barrier_semaphore()
    for d in range(1, n):
        pl.semaphore_signal(
            barrier, inc=1, device_id=(lax.rem(me + d, n), t), device_id_type=MESH
        )
    for d in range(2, tp, 2):
        for m in range(a):
            pl.semaphore_signal(
                barrier, inc=1, device_id=(beta * a + m, lax.rem(t + d, tp)),
                device_id_type=MESH,
            )
    pl.semaphore_signal(barrier, inc=1, device_id=(me, partner), device_id_type=MESH)

    loads = [
        pltpu.make_async_copy(src, dst, ld.at[i])
        for i, (src, dst) in enumerate(
            [(chosen_ref, ch_v), (k_ref, k_in), (v_ref, v_in), (q_ref, q_in), (g_ref, g_in)]
            + (
                [(x_ref, x_in)]
                if width % 128
                else [
                    (x_ref.at[:, q * width : (q + 1) * width], xst.at[q])
                    for q in range(n_chunk)
                ]
            )
        )
    ]
    for c in loads:
        c.start()

    loads[0].wait()
    picked = ch_v[...]
    ids = lax.broadcasted_iota(jnp.int32, sel_v.shape, 1)
    hit = jnp.zeros(sel_v.shape, jnp.int32)
    for s in range(picked.shape[1]):
        hit = jnp.where(picked[:, s : s + 1] == ids, 1, hit)
    sel_v[...] = hit
    to_scalar = pltpu.make_async_copy(sel_v, sel_s, ld.at[len(loads)])
    to_scalar.start()

    def head_cols(h):
        return slice(h * HEAD_SIZE, (h + 1) * HEAD_SIZE)

    loads[1].wait()
    loads[2].wait()
    for h in range(heads):
        for blk in range(owner):
            at = slice(blk * KB, (blk + 1) * KB)
            kvown[h, blk, :, 0:HEAD_SIZE] = k_in[at, head_cols(h)]
            kvown[h, blk, :, HEAD_SIZE : 2 * HEAD_SIZE] = v_in[at, head_cols(h)]
    to_scalar.wait()

    def used_blocks(i, j):
        used = []
        for blk in range(owner):
            u = sel_s[i * local, j * owner + blk]
            for r in range(1, local):
                u = jnp.maximum(u, sel_s[i * local + r, j * owner + blk])
            used.append(u)
        return used

    def slots(i, j):
        used = used_blocks(i, j)
        picks = []
        for p in range(local):
            before = jnp.int32(0)
            one = []
            for blk in range(owner):
                one.append(jnp.where(before == p, used[blk], 0))
                before = before + used[blk]
            picks.append(one)
        return picks

    def kv_copy(h, i, j):
        return remote(kvst.at[h, i], kvbuf.at[h, j], kv_send.at[h, i], kv_recv.at[h, j], i, t)

    def stage_kv(ii, carry):
        i = n - 1 - ii
        picks = slots(i, me)
        for p in range(local):
            at = jnp.int32(0)
            for blk in range(owner):
                at = at + picks[p][blk] * blk
            for h in range(heads):
                kvst[h, i, p * KB : (p + 1) * KB, :] = kvown[h, at]
        return carry

    lax.fori_loop(0, n - 1 - me, stage_kv, 0)

    pl.semaphore_wait(barrier, n + (tp // 2 - 1) * a)

    for h in range(heads):

        def start_kv(ii, carry):
            kv_copy(h, n - 1 - ii, me).start()
            return carry

        lax.fori_loop(0, n - 1 - me, start_kv, 0)

    for c in loads[5:]:
        c.wait()
    if width % 128:
        for q in range(n_chunk):
            xst[q] = x_in[:, q * width : (q + 1) * width]

    def x_copy(q, y):
        c = t * n_chunk + q
        return remote(
            xst.at[q], xbuf.at[alpha, lax.div(c, a)], x_send.at[q, y],
            x_recv.at[alpha, lax.div(c, a)], beta * a + lax.rem(c, a), 2 * y + parity,
        )

    def x_mine(q, y):
        return jnp.logical_and(lax.rem(t * n_chunk + q, a) == alpha, t == 2 * y + parity)

    for q in range(n_chunk):
        c = t * n_chunk + q
        for y in range(tp // 2):

            @pl.when(jnp.logical_not(x_mine(q, y)))
            def _():
                x_copy(q, y).start()

            @pl.when(x_mine(q, y))
            def _():
                xbuf[alpha, lax.div(c, a)] = xst[q]

    loads[3].wait()
    loads[4].wait()
    for h in range(heads):
        for gr in range(group):
            hh = h * group + gr
            at = slice(gr * rows, (gr + 1) * rows)
            qz[h, at, 0:HEAD_SIZE] = (q_in[:, head_cols(hh)].astype(F32) * scale).astype(BF16)
            qz[h, at, HEAD_SIZE : 2 * HEAD_SIZE] = jnp.zeros((rows, HEAD_SIZE), BF16)
            gz[h, at, 0:HEAD_SIZE] = jnp.zeros((rows, HEAD_SIZE), BF16)
            gz[h, at, HEAD_SIZE : 2 * HEAD_SIZE] = g_in[:, head_cols(hh)]

    lane = lax.broadcasted_iota(jnp.int32, (1, rows), 1)
    lane_block = lax.div(lane, QB)

    def row_bias(flags):
        vals = [jnp.where(f > 0, F32(0.0), F32(NEG)) for f in flags]
        out = jnp.full((1, rows), vals[0], F32)
        for r in range(1, local):
            out = jnp.where(lane_block == r, vals[r], out)
        return out

    def own_bias():
        return [
            row_bias([sel_s[me * local + r, me * owner + blk] for r in range(local)])
            for blk in range(owner)
        ]

    def far_bias(j):
        picks = slots(me, j)
        out = []
        for p in range(local):
            flags = []
            for r in range(local):
                f = jnp.int32(0)
                for blk in range(owner):
                    f = f + picks[p][blk] * sel_s[me * local + r, j * owner + blk]
                flags.append(f)
            out.append(row_bias(flags))
        return out

    def tile(gr):
        return slice(gr * rows, (gr + 1) * rows)

    def g_copy(h, i, j):
        return remote(gst.at[h, j], grecv.at[h, i], g_send.at[h, j], g_recv.at[h, i], j, t)

    def q_copy(h, m):
        return remote(
            qall.at[h, alpha], qall.at[h, alpha], q_send.at[h, m], q_recv.at[h, alpha],
            beta * a + m, t,
        )

    def w_copy(h, bb):
        return remote(
            wst.at[h, bb], wrecv.at[h, beta], w_send.at[h, bb], w_recv.at[h, beta],
            bb * a + alpha, t,
        )

    def first_pass(h, kv, base, idx, bias, causal, stats):
        size = kv.shape[0]
        out = []
        for gr in range(group):
            m, l, rd = stats[gr]
            s = dot_nt(kv, qz[h, tile(gr), :])
            parts = []
            for p in range(size // KB):
                part = s[p * KB : (p + 1) * KB] + bias[p]
                if causal:
                    key = p * KB + lax.broadcasted_iota(jnp.int32, (KB, rows), 0)
                    part = jnp.where(key <= lane, part, NEG)
                parts.append(part)
            s = jnp.concatenate(parts, axis=0)
            mj = jnp.maximum(m, jnp.max(s, axis=0, keepdims=True))
            e = jnp.exp(s - mj)
            dp = dot_nt(kv, gz[h, tile(gr), :])
            e_buf[pl.ds(base, size), tile(gr)] = e
            dp_buf[pl.ds(base, size), tile(gr)] = dp
            mj_buf[idx, :, tile(gr)] = mj
            back = jnp.exp(m - mj)
            l = l * back + jnp.sum(e, axis=0, keepdims=True)
            rd = rd * back + jnp.sum(e * dp, axis=0, keepdims=True)
            out.append((mj, l, rd))
        return tuple(out)

    def second_pass(h, kv, base, idx, stats, first):
        size = kv.shape[0]
        keys = kv[:, 0:HEAD_SIZE]
        out = None
        for gr in range(group):
            m, inv, rd = stats[gr]
            f = jnp.exp(mj_buf[idx, :, tile(gr)] - m) * inv
            p = e_buf[pl.ds(base, size), tile(gr)] * f
            ds = (p * (dp_buf[pl.ds(base, size), tile(gr)] - rd)).astype(BF16)
            term = dot_nn(ds, qz[h, tile(gr), :]) + dot_nn(p.astype(BF16), gz[h, tile(gr), :])
            out = term if out is None else out + term
            dq = dot_tn(keys, ds)
            if first:
                dqt[:, tile(gr)] = dq
            else:
                dqt[:, tile(gr)] += dq
        return out

    odd = lax.rem(me, 2)
    pairs = lax.div(me, 2)

    def own_kv(h):
        return jnp.concatenate([kvown[h, blk] for blk in range(owner)], axis=0)

    def pair_kv(h, jj):
        return jnp.concatenate([kvbuf[h, 2 * jj], kvbuf[h, 2 * jj + 1]], axis=0)

    def attend(h):
        none = jnp.full((1, rows), NEG, F32)
        zero = jnp.zeros((1, rows), F32)
        stats = first_pass(
            h, own_kv(h), 0, 0, own_bias(), True, ((none, zero, zero),) * group
        )

        def one_single(_, stats):
            j = me - 1
            kv_copy(h, j, j).wait_recv()
            return first_pass(h, kvbuf[h, j], single_at, 1, far_bias(j), False, stats)

        stats = lax.fori_loop(0, odd, one_single, stats)

        def one_pair(ii, stats):
            jj = pairs - 1 - ii
            for d in range(2):
                kv_copy(h, 2 * jj + d, 2 * jj + d).wait_recv()
            base = pl.multiple_of(pair_at + jj * (2 * chunk), chunk)
            bias = far_bias(2 * jj) + far_bias(2 * jj + 1)
            return first_pass(h, pair_kv(h, jj), base, 2 + jj, bias, False, stats)

        stats = lax.fori_loop(0, pairs, one_pair, stats)
        fin = []
        for m, l, rd in stats:
            inv = 1.0 / l
            fin.append((m, inv, rd * inv))

        own_acc[h] = second_pass(h, own_kv(h), 0, 0, fin, True)

        def back_pair(jj, carry):
            base = pl.multiple_of(pair_at + jj * (2 * chunk), chunk)
            out = second_pass(h, pair_kv(h, jj), base, 2 + jj, fin, False).astype(BF16)
            for d in range(2):
                gst[h, 2 * jj + d] = out[d * chunk : (d + 1) * chunk]
            for d in range(2):
                g_copy(h, me, 2 * jj + d).start()
            return carry

        lax.fori_loop(0, pairs, back_pair, 0)

        def back_single(_, carry):
            j = me - 1
            gst[h, j] = second_pass(h, kvbuf[h, j], single_at, 1, fin, False).astype(BF16)
            g_copy(h, me, j).start()
            return carry

        lax.fori_loop(0, odd, back_single, 0)

        stacked = jnp.concatenate([dqt[:, tile(gr)] for gr in range(group)], axis=0)
        part = (stacked * scale).T.astype(BF16)
        qall[h, alpha] = part
        dq_ref[:, h * gcols : (h + 1) * gcols] = part
        for mm in range(a):

            @pl.when(alpha != mm)
            def _():
                q_copy(h, mm).start()

    def x_direct(bb):
        return lax.rem(lax.div(bb * a + alpha, n_chunk), 2) == parity

    def x_at_home(m, bb):
        return jnp.logical_and(alpha == m, lax.div(bb * a + alpha, n_chunk) == t)

    def x_here(m, bb):
        return remote(
            xst.at[0], xbuf.at[m, bb], x_send.at[0, 0], x_recv.at[m, bb], me, t
        )

    def x_forward(m, bb):
        return remote(
            xbuf.at[m, bb], xbuf.at[m, bb], f_send.at[m, bb], x_recv.at[m, bb], me, partner
        )

    def relay_x():
        for bb in range(b):
            for m in range(a):

                @pl.when(x_direct(bb))
                def _():
                    @pl.when(jnp.logical_not(x_at_home(m, bb)))
                    def _():
                        x_here(m, bb).wait_recv()

                    x_forward(m, bb).start()

    def gather_x():
        for bb in range(b):
            for m in range(a):

                @pl.when(jnp.logical_not(x_direct(bb)))
                def _():
                    x_here(m, bb).wait_recv()

    def weight_part(h):
        for mm in range(a):

            @pl.when(alpha != mm)
            def _():
                remote(
                    qall.at[h, mm], qall.at[h, mm], q_send.at[h, mm], q_recv.at[h, mm], me, t
                ).wait_recv()

        def partial(bb):
            out = dot_tn(xbuf[0, bb], qall[h, 0])
            for m in range(1, a):
                out = out + dot_tn(xbuf[m, bb], qall[h, m])
            return out

        for d in range(1, b):
            bb = lax.rem(beta + d, b)
            wst[h, bb] = partial(bb).astype(BF16)
            w_copy(h, bb).start()
        w_own[h] = partial(beta)

    for h in range(heads):
        attend(h)
        if h == 0:
            relay_x()
    gather_x()
    for h in range(heads):
        weight_part(h)

    for h in range(heads):

        def add_far(i, carry):
            remote(gst.at[h, 0], grecv.at[h, i], g_send.at[h, 0], g_recv.at[h, i], me, t).wait_recv()
            picks = slots(i, me)
            for p in range(local):
                got = grecv[h, i, p * KB : (p + 1) * KB, :].astype(F32)
                for blk in range(owner):
                    own_acc[h, blk * KB : (blk + 1) * KB, :] += jnp.where(
                        picks[p][blk] > 0, got, 0.0
                    )
            return carry

        lax.fori_loop(me + 1, n, add_far, 0)
        dk_ref[:, head_cols(h)] = own_acc[h, :, 0:HEAD_SIZE].astype(BF16)
        dv_ref[:, head_cols(h)] = own_acc[h, :, HEAD_SIZE : 2 * HEAD_SIZE].astype(BF16)

    for h in range(heads):
        total = w_own[h]
        for d in range(1, b):
            bb = lax.rem(beta + d, b)
            remote(
                wst.at[h, bb], wrecv.at[h, bb], w_send.at[h, bb], w_recv.at[h, bb], me, t
            ).wait_recv()
            total = total + wrecv[h, bb].astype(F32)
        w_ref[:, h * gcols : (h + 1) * gcols] = total

    for h in range(heads):

        def done_kv(i, carry):
            kv_copy(h, i, me).wait_send()
            return carry

        lax.fori_loop(me + 1, n, done_kv, 0)
    for q in range(n_chunk):
        for y in range(tp // 2):

            @pl.when(jnp.logical_not(x_mine(q, y)))
            def _():
                x_copy(q, y).wait_send()

    for bb in range(b):
        for m in range(a):

            @pl.when(x_direct(bb))
            def _():
                x_forward(m, bb).wait_send()

    for h in range(heads):

        def done_g(j, carry):
            g_copy(h, me, j).wait_send()
            return carry

        lax.fori_loop(0, me, done_g, 0)
        for mm in range(a):

            @pl.when(alpha != mm)
            def _():
                q_copy(h, mm).wait_send()

        for d in range(1, b):
            w_copy(h, lax.rem(beta + d, b)).wait_send()


def write_out(*refs):
    count = (len(refs) - 1) // 2
    sems = refs[-1]
    copies = [
        pltpu.make_async_copy(refs[i], refs[count + i], sems.at[i]) for i in range(count)
    ]
    for c in copies:
        c.start()
    for c in copies:
        c.wait()


def body(n, tp, inputs, queries, key_vectors, value_rows_by_head, out_grad, chosen):
    rows, cols = key_vectors.shape
    q_cols = queries.shape[1]
    heads = cols // HEAD_SIZE
    group = q_cols // cols
    local = rows // QB
    chunk = local * KB
    wide = group * rows
    d_model = inputs.shape[1] * tp
    width = d_model // n
    n_chunk = inputs.shape[1] // width
    a = 4
    b = n // a
    gcols = group * HEAD_SIZE
    blocks = n * rows // KB
    lanes = -(-blocks // 128) * 128
    keys = rows + chunk + (n // 2) * 2 * chunk
    vmem = pl.BlockSpec(memory_space=pltpu.VMEM)
    hbm = pl.BlockSpec(memory_space=pl.ANY)
    dma = pltpu.SemaphoreType.DMA
    outs = (
        ((rows, q_cols), BF16),
        ((rows, cols), BF16),
        ((rows, cols), BF16),
        ((width, q_cols), F32),
    )
    held = pl.pallas_call(
        functools.partial(kernel, n, tp, a, b),
        out_shape=tuple(pltpu.VMEM(s, d) for s, d in outs),
        in_specs=[hbm] * 6,
        out_specs=(vmem,) * 4,
        scratch_shapes=[
            pltpu.VMEM(chosen.shape, jnp.int32),
            pltpu.VMEM((chosen.shape[0], lanes), jnp.int32),
            pltpu.SMEM((chosen.shape[0], lanes), jnp.int32),
            pltpu.VMEM(inputs.shape, BF16),
            pltpu.VMEM((n_chunk, rows, width), BF16),
            pltpu.VMEM((rows, q_cols), BF16),
            pltpu.VMEM((rows, q_cols), BF16),
            pltpu.VMEM((rows, cols), BF16),
            pltpu.VMEM((rows, cols), BF16),
            pltpu.VMEM((heads, wide, 2 * HEAD_SIZE), BF16),
            pltpu.VMEM((heads, wide, 2 * HEAD_SIZE), BF16),
            pltpu.VMEM((heads, rows // KB, KB, 2 * HEAD_SIZE), BF16),
            pltpu.VMEM((heads, n, chunk, 2 * HEAD_SIZE), BF16),
            pltpu.VMEM((heads, n, chunk, 2 * HEAD_SIZE), BF16),
            pltpu.VMEM((a, b, rows, width), BF16),
            pltpu.VMEM((keys, wide), F32),
            pltpu.VMEM((keys, wide), F32),
            pltpu.VMEM((2 + n // 2, 1, wide), F32),
            pltpu.VMEM((HEAD_SIZE, wide), F32),
            pltpu.VMEM((heads, n, chunk, 2 * HEAD_SIZE), BF16),
            pltpu.VMEM((heads, n, chunk, 2 * HEAD_SIZE), BF16),
            pltpu.VMEM((heads, rows, 2 * HEAD_SIZE), F32),
            pltpu.VMEM((heads, a, rows, gcols), BF16),
            pltpu.VMEM((heads, b, width, gcols), BF16),
            pltpu.VMEM((heads, b, width, gcols), BF16),
            pltpu.VMEM((heads, width, gcols), F32),
            dma((6 + n_chunk,)),
            dma((heads, n)),
            dma((heads, n)),
            dma((n_chunk, tp // 2)),
            dma((a, b)),
            dma((a, b)),
            dma((heads, n)),
            dma((heads, n)),
            dma((heads, a)),
            dma((heads, a)),
            dma((heads, b)),
            dma((heads, b)),
        ],
        compiler_params=pltpu.CompilerParams(
            collective_id=0, has_side_effects=True, vmem_limit_bytes=58 * 1024 * 1024
        ),
    )(chosen, inputs, queries, key_vectors, value_rows_by_head, out_grad)
    return pl.pallas_call(
        write_out,
        out_shape=tuple(jax.ShapeDtypeStruct(s, d) for s, d in outs),
        in_specs=[vmem] * 4,
        out_specs=(hbm,) * 4,
        scratch_shapes=[dma((4,))],
        compiler_params=pltpu.CompilerParams(vmem_limit_bytes=1024 * 1024),
    )(*held)


def solution(mesh):
    n, tp = mesh.shape["kv"], mesh.shape["tp"]
    placed = (P("kv", "tp"),) * 5 + (P(),)
    return jax.shard_map(
        functools.partial(body, n, tp),
        mesh=mesh,
        in_specs=placed,
        out_specs=(P("kv", "tp"),) * 4,
        check_vma=False,
    )
```

```python
import functools

import jax
import jax.numpy as jnp
from jax import lax
from jax.experimental import pallas as pl
from jax.experimental.pallas import tpu as pltpu
from jax.sharding import PartitionSpec as P

HEAD_SIZE = 64
QB = 128
KB = 64
NEG = -1e30
PARTS = 2
BF16 = jnp.bfloat16
F32 = jnp.float32
MESH = pl.DeviceIdType.MESH


def dot_nt(x, y):
    return lax.dot_general(x, y, (((1,), (1,)), ((), ())), preferred_element_type=F32)


def dot_nn(x, y):
    return lax.dot_general(x, y, (((1,), (0,)), ((), ())), preferred_element_type=F32)


def dot_tn(x, y):
    return lax.dot_general(x, y, (((0,), (0,)), ((), ())), preferred_element_type=F32)


def kernel(
    n, tp, a, b,
    chosen_ref, x_ref, q_ref, k_ref, v_ref, g_ref,
    dq_ref, dk_ref, dv_ref, w_ref,
    ch_v, sel_v, sel_s, x_in, xst, q_in, g_in, k_in, v_in, qz, gz, kvown, kvst, kvbuf, xbuf, xt,
    e_buf, dp_buf, mj_buf, dqt, gst, grecv, own_acc, qall, wst, wrecv, w_own,
    ld, kv_send, kv_recv, x_send, x_recv, f_send, g_send, g_recv, q_send, q_recv,
    w_send, w_recv, pair_sem,
):
    me = lax.axis_index("kv")
    t = lax.axis_index("tp")
    alpha = lax.rem(me, a)
    beta = lax.div(me, a)
    parity = lax.rem(t, 2)
    partner = t + 1 - 2 * parity

    def flip(m, step):
        for bit in (1, 2):
            if step & bit:
                m = m + bit - 2 * bit * lax.rem(lax.div(m, bit), 2)
        return m

    rows, cols = k_in.shape
    heads = cols // HEAD_SIZE
    group = q_in.shape[1] // cols
    local = rows // QB
    owner = rows // KB
    chunk = local * KB
    wide = group * rows
    width = xst.shape[2]
    n_chunk = xst.shape[0]
    parts = qall.shape[0] // heads
    ucols = qall.shape[3]
    scale = HEAD_SIZE ** (-0.5)
    single_at = heads * rows
    pair_at = single_at + chunk

    def remote(src, dst, send, recv, kv, tpi):
        return pltpu.make_async_remote_copy(
            src_ref=src, dst_ref=dst, send_sem=send, recv_sem=recv,
            device_id=(kv, tpi), device_id_type=MESH,
        )

    barrier = pltpu.get_barrier_semaphore()
    for d in range(1, n):
        pl.semaphore_signal(
            barrier, inc=1, device_id=(lax.rem(me + d, n), t), device_id_type=MESH
        )
    for d in range(2, tp, 2):
        pl.semaphore_signal(
            barrier, inc=1, device_id=(me, lax.rem(t + d, tp)), device_id_type=MESH
        )
    pl.semaphore_signal(barrier, inc=1, device_id=(me, partner), device_id_type=MESH)

    loads = [
        pltpu.make_async_copy(src, dst, ld.at[i])
        for i, (src, dst) in enumerate(
            [(chosen_ref, ch_v), (k_ref, k_in), (v_ref, v_in), (q_ref, q_in), (g_ref, g_in)]
            + (
                [(x_ref, x_in)]
                if width % 128
                else [
                    (x_ref.at[:, q * width : (q + 1) * width], xst.at[q])
                    for q in range(n_chunk)
                ]
            )
        )
    ]
    for c in loads:
        c.start()

    loads[0].wait()
    picked = ch_v[...]
    ids = lax.broadcasted_iota(jnp.int32, sel_v.shape, 1)
    hit = jnp.zeros(sel_v.shape, jnp.int32)
    for s in range(picked.shape[1]):
        hit = jnp.where(picked[:, s : s + 1] == ids, 1, hit)
    sel_v[...] = hit
    to_scalar = pltpu.make_async_copy(sel_v, sel_s, ld.at[len(loads)])
    to_scalar.start()

    def head_cols(h):
        return slice(h * HEAD_SIZE, (h + 1) * HEAD_SIZE)

    loads[1].wait()
    loads[2].wait()
    for h in range(heads):
        for blk in range(owner):
            at = slice(blk * KB, (blk + 1) * KB)
            kvown[h, blk, :, 0:HEAD_SIZE] = k_in[at, head_cols(h)]
            kvown[h, blk, :, HEAD_SIZE : 2 * HEAD_SIZE] = v_in[at, head_cols(h)]
    to_scalar.wait()

    def used_blocks(i, j):
        used = []
        for blk in range(owner):
            u = sel_s[i * local, j * owner + blk]
            for r in range(1, local):
                u = jnp.maximum(u, sel_s[i * local + r, j * owner + blk])
            used.append(u)
        return used

    def slots(i, j):
        used = used_blocks(i, j)
        picks = []
        for p in range(local):
            before = jnp.int32(0)
            one = []
            for blk in range(owner):
                one.append(jnp.where(before == p, used[blk], 0))
                before = before + used[blk]
            picks.append(one)
        return picks

    def kv_copy(h, i, j):
        return remote(kvst.at[h, i], kvbuf.at[h, j], kv_send.at[h, i], kv_recv.at[h, j], i, t)

    def stage_kv(ii, carry):
        i = n - 1 - ii
        picks = slots(i, me)
        for p in range(local):
            at = jnp.int32(0)
            for blk in range(owner):
                at = at + picks[p][blk] * blk
            for h in range(heads):
                kvst[h, i, p * KB : (p + 1) * KB, :] = kvown[h, at]
        return carry

    lax.fori_loop(0, n - 1 - me, stage_kv, 0)

    pl.semaphore_wait(barrier, n + tp // 2 - 1)

    def send_kv(h):
        def start_kv(ii, carry):
            kv_copy(h, n - 1 - ii, me).start()
            return carry

        lax.fori_loop(0, n - 1 - me, start_kv, 0)

    send_kv(0)

    for c in loads[5:]:
        c.wait()
    if width % 128:
        for q in range(n_chunk):
            xst[q] = x_in[:, q * width : (q + 1) * width]

    def x_copy(q):
        c = t * n_chunk + q
        return remote(
            xst.at[q], xbuf.at[alpha, lax.div(c, a)], x_send.at[q],
            x_recv.at[alpha, lax.div(c, a)], beta * a + lax.rem(c, a), t,
        )

    def send_x(late):
        for q in range(n_chunk):
            c = t * n_chunk + q
            ahead = lax.rem(c, a) - alpha

            @pl.when(ahead > 1 if late else jnp.logical_and(ahead < 2, ahead != 0))
            def _():
                x_copy(q).start()

            if not late:

                @pl.when(ahead == 0)
                def _():
                    xbuf[alpha, lax.div(c, a)] = xst[q]

    loads[3].wait()
    loads[4].wait()
    for h in range(heads):
        for gr in range(group):
            hh = h * group + gr
            at = slice(gr * rows, (gr + 1) * rows)
            qz[h, at, 0:HEAD_SIZE] = (q_in[:, head_cols(hh)].astype(F32) * scale).astype(BF16)
            qz[h, at, HEAD_SIZE : 2 * HEAD_SIZE] = jnp.zeros((rows, HEAD_SIZE), BF16)
            gz[h, at, 0:HEAD_SIZE] = jnp.zeros((rows, HEAD_SIZE), BF16)
            gz[h, at, HEAD_SIZE : 2 * HEAD_SIZE] = g_in[:, head_cols(hh)]

    lane = lax.broadcasted_iota(jnp.int32, (1, rows), 1)
    lane_block = lax.div(lane, QB)

    def row_bias(flags):
        vals = [jnp.where(f > 0, F32(0.0), F32(NEG)) for f in flags]
        out = jnp.full((1, rows), vals[0], F32)
        for r in range(1, local):
            out = jnp.where(lane_block == r, vals[r], out)
        return out

    def own_bias():
        return [
            row_bias([sel_s[me * local + r, me * owner + blk] for r in range(local)])
            for blk in range(owner)
        ]

    def far_bias(j):
        picks = slots(me, j)
        out = []
        for p in range(local):
            flags = []
            for r in range(local):
                f = jnp.int32(0)
                for blk in range(owner):
                    f = f + picks[p][blk] * sel_s[me * local + r, j * owner + blk]
                flags.append(f)
            out.append(row_bias(flags))
        return out

    def tile(gr):
        return slice(gr * rows, (gr + 1) * rows)

    def g_copy(h, i, j):
        return remote(gst.at[h, j], grecv.at[h, i], g_send.at[h, j], g_recv.at[h, i], j, t)

    def hop(u):
        return 1 + u % 2

    def q_send_to(h, m, step):
        own = m is alpha
        return remote(
            qall.at[h, m], qall.at[h, m], q_send.at[h, step if own else 0], q_recv.at[h, m],
            beta * a + flip(alpha, step), t,
        )

    def q_here(h, m):
        return remote(qall.at[h, m], qall.at[h, m], q_send.at[h, 0], q_recv.at[h, m], me, t)

    def relay_q(u):
        m = flip(alpha, 3 - hop(u))
        q_here(u, m).wait_recv()
        q_send_to(u, m, hop(u)).start()

    def w_copy(h, bb):
        return remote(
            wst.at[h, bb], wrecv.at[h, beta], w_send.at[h, bb], w_recv.at[h, beta],
            bb * a + alpha, t,
        )

    def first_pass(h, kv, base, idx, bias, causal, stats):
        size = kv.shape[0]
        out = []
        for gr in range(group):
            m, l, rd = stats[gr]
            s = dot_nt(kv, qz[h, tile(gr), :])
            rows_of = []
            for p in range(size // KB):
                part = s[p * KB : (p + 1) * KB] + bias[p]
                if causal:
                    key = p * KB + lax.broadcasted_iota(jnp.int32, (KB, rows), 0)
                    part = jnp.where(key <= lane, part, NEG)
                rows_of.append(part)
            s = jnp.concatenate(rows_of, axis=0)
            mj = jnp.maximum(m, jnp.max(s, axis=0, keepdims=True))
            e = jnp.exp(s - mj)
            dp = dot_nt(kv, gz[h, tile(gr), :])
            e_buf[pl.ds(base, size), tile(gr)] = e
            dp_buf[pl.ds(base, size), tile(gr)] = dp
            mj_buf[idx, :, tile(gr)] = mj
            back = jnp.exp(m - mj)
            l = l * back + jnp.sum(e, axis=0, keepdims=True)
            rd = rd * back + jnp.sum(e * dp, axis=0, keepdims=True)
            out.append((mj, l, rd))
        return tuple(out)

    def second_pass(h, kv, base, idx, stats, first):
        size = kv.shape[0]
        keys = kv[:, 0:HEAD_SIZE]
        out = None
        for gr in range(group):
            m, inv, rd = stats[gr]
            f = jnp.exp(mj_buf[idx, :, tile(gr)] - m) * inv
            p = e_buf[pl.ds(base, size), tile(gr)] * f
            ds = (p * (dp_buf[pl.ds(base, size), tile(gr)] - rd)).astype(BF16)
            term = dot_nn(ds, qz[h, tile(gr), :]) + dot_nn(p.astype(BF16), gz[h, tile(gr), :])
            out = term if out is None else out + term
            dq = dot_tn(keys, ds)
            if first:
                dqt[:, tile(gr)] = dq
            else:
                dqt[:, tile(gr)] += dq
        return out

    odd = lax.rem(me, 2)
    pairs = lax.div(me, 2)

    def own_kv(h):
        return jnp.concatenate([kvown[h, blk] for blk in range(owner)], axis=0)

    def pair_kv(h, jj):
        return jnp.concatenate([kvbuf[h, 2 * jj], kvbuf[h, 2 * jj + 1]], axis=0)

    state = {}

    def own(h):
        none = jnp.full((1, rows), NEG, F32)
        zero = jnp.zeros((1, rows), F32)
        state[h] = first_pass(
            h, own_kv(h), h * rows, h, own_bias(), True, ((none, zero, zero),) * group
        )

    def far(h):
        def one_single(_, stats):
            j = me - 1
            kv_copy(h, j, j).wait_recv()
            return first_pass(h, kvbuf[h, j], single_at, heads, far_bias(j), False, stats)

        stats = state[h]
        stats = lax.fori_loop(0, odd, one_single, stats)

        def one_pair(ii, stats):
            jj = pairs - 1 - ii
            for d in range(2):
                kv_copy(h, 2 * jj + d, 2 * jj + d).wait_recv()
            base = pl.multiple_of(pair_at + jj * (2 * chunk), chunk)
            bias = far_bias(2 * jj) + far_bias(2 * jj + 1)
            return first_pass(h, pair_kv(h, jj), base, heads + 1 + jj, bias, False, stats)

        stats = lax.fori_loop(0, pairs, one_pair, stats)
        fin = []
        for m, l, rd in stats:
            inv = 1.0 / l
            fin.append((m, inv, rd * inv))
        state[h] = fin

    def back(h):
        fin = state[h]
        own_acc[h] = second_pass(h, own_kv(h), h * rows, h, fin, True)

        def back_pair(jj, carry):
            base = pl.multiple_of(pair_at + jj * (2 * chunk), chunk)
            out = second_pass(h, pair_kv(h, jj), base, heads + 1 + jj, fin, False).astype(BF16)
            for d in range(2):
                gst[h, 2 * jj + d] = out[d * chunk : (d + 1) * chunk]
            return carry

        lax.fori_loop(0, pairs, back_pair, 0)

        def back_single(_, carry):
            j = me - 1
            gst[h, j] = second_pass(h, kvbuf[h, j], single_at, heads, fin, False).astype(BF16)
            return carry

        lax.fori_loop(0, odd, back_single, 0)

        per = group // parts
        for u in range(parts):
            stacked = jnp.concatenate(
                [dqt[:, tile(gr)] for gr in range(u * per, (u + 1) * per)], axis=0
            )
            part = (stacked * scale).T.astype(BF16)
            at = h * parts + u
            qall[at, alpha] = part
            dq_ref[:, at * ucols : (at + 1) * ucols] = part
            for step in (2, 1):
                q_send_to(at, alpha, step).start()

    def send_g(h):
        def start_g(j, carry):
            g_copy(h, me, j).start()
            return carry

        lax.fori_loop(0, me, start_g, 0)

    def x_source(bb):
        return lax.div(bb * a + alpha, n_chunk)

    def x_here(m, bb):
        return remote(xst.at[0], xbuf.at[m, bb], x_send.at[0], x_recv.at[m, bb], me, t)

    def x_forward(m, bb, d):
        to = partner if d == 0 else lax.rem(t + 2 * d, tp)
        return remote(
            xbuf.at[m, bb], xbuf.at[m, bb], f_send.at[m, bb, d], x_recv.at[m, bb], me, to
        )

    def relay_x(step):
        m = flip(alpha, step)
        for bb in range(b):

            @pl.when(x_source(bb) == t)
            def _():
                if step:
                    x_here(m, bb).wait_recv()
                for d in range(tp // 2 - 1, -1, -1):
                    x_forward(m, bb, d).start()

    def relay_far(early):
        lower = lax.rem(lax.div(alpha, 2), 2) == 0

        @pl.when(lower if early else jnp.logical_not(lower))
        def _():
            relay_x(2)
            relay_x(3)

    def gather_x():
        for step in range(a):
            m = flip(alpha, step)
            for bb in range(b):
                src = x_source(bb)

                @pl.when(src != t)
                def _():
                    x_here(m, bb).wait_recv()

                @pl.when(jnp.logical_and(src != t, lax.rem(src, 2) == parity))
                def _():
                    x_forward(m, bb, 0).start()

        for bb in range(b):
            for m in range(a):
                xt[m, bb] = xbuf[m, bb].T

    def weight_part(h):
        q_here(h, flip(alpha, hop(h))).wait_recv()
        q_here(h, flip(alpha, 3)).wait_recv()

        def partial(bb):
            out = dot_nn(xt[0, bb], qall[h, 0])
            for m in range(1, a):
                out = out + dot_nn(xt[m, bb], qall[h, m])
            return out

        for d in range(1, b):
            bb = lax.rem(beta + d, b)
            wst[h, bb] = partial(bb).astype(BF16)
            w_copy(h, bb).start()
        w_own[h] = partial(beta)

    def wait_kv(h):
        def done_kv(i, carry):
            kv_copy(h, i, me).wait_send()
            return carry

        lax.fori_loop(me + 1, n, done_kv, 0)

    own(0)
    wait_kv(0)
    pl.semaphore_signal(pair_sem, inc=1, device_id=(me, partner), device_id_type=MESH)
    if heads > 1:
        own(1)
    pl.semaphore_wait(pair_sem, 1)
    for h in range(1, heads):
        send_kv(h)
    send_x(False)
    far(0)
    back(0)
    send_g(0)
    send_x(True)
    relay_x(0)
    relay_x(1)
    relay_far(True)
    for h in range(1, heads):
        if h > 1:
            own(h)
        far(h)
        for u in range((h - 1) * parts, h * parts):
            relay_q(u)
        back(h)
        send_g(h)
    relay_far(False)
    gather_x()
    last = (heads - 1) * parts
    for u in range(last):
        weight_part(u)
    for u in range(last, heads * parts):
        relay_q(u)
    for u in range(last, heads * parts):
        weight_part(u)

    for h in range(heads):

        def add_far(i, carry):
            remote(gst.at[h, 0], grecv.at[h, i], g_send.at[h, 0], g_recv.at[h, i], me, t).wait_recv()
            picks = slots(i, me)
            for p in range(local):
                got = grecv[h, i, p * KB : (p + 1) * KB, :].astype(F32)
                for blk in range(owner):
                    own_acc[h, blk * KB : (blk + 1) * KB, :] += jnp.where(
                        picks[p][blk] > 0, got, 0.0
                    )
            return carry

        lax.fori_loop(me + 1, n, add_far, 0)
        dk_ref[:, head_cols(h)] = own_acc[h, :, 0:HEAD_SIZE].astype(BF16)
        dv_ref[:, head_cols(h)] = own_acc[h, :, HEAD_SIZE : 2 * HEAD_SIZE].astype(BF16)

    def wait_w(h):
        total = w_own[h]
        for d in range(1, b):
            bb = lax.rem(beta + d, b)
            remote(
                wst.at[h, bb], wrecv.at[h, bb], w_send.at[h, bb], w_recv.at[h, bb], me, t
            ).wait_recv()
            total = total + wrecv[h, bb].astype(F32)
        w_ref[:, h * ucols : (h + 1) * ucols] = total

    for h in range(heads * parts):
        wait_w(h)

    for h in range(1, heads):
        wait_kv(h)
    for q in range(n_chunk):

        @pl.when(lax.rem(t * n_chunk + q, a) != alpha)
        def _():
            x_copy(q).wait_send()

    for bb in range(b):
        src = x_source(bb)
        for m in range(a):

            @pl.when(lax.rem(src, 2) == parity)
            def _():
                x_forward(m, bb, 0).wait_send()

            @pl.when(src == t)
            def _():
                for d in range(1, tp // 2):
                    x_forward(m, bb, d).wait_send()

    for h in range(heads):

        def done_g(j, carry):
            g_copy(h, me, j).wait_send()
            return carry

        lax.fori_loop(0, me, done_g, 0)

    for u in range(heads * parts):
        for step in (2, 1):
            q_send_to(u, alpha, step).wait_send()
        q_send_to(u, flip(alpha, 3 - hop(u)), hop(u)).wait_send()
        for d in range(1, b):
            w_copy(u, lax.rem(beta + d, b)).wait_send()


def write_out(*refs):
    count = (len(refs) - 1) // 2
    sems = refs[-1]
    copies = [
        pltpu.make_async_copy(refs[i], refs[count + i], sems.at[i]) for i in range(count)
    ]
    for c in copies:
        c.start()
    for c in copies:
        c.wait()


def body(n, tp, inputs, queries, key_vectors, value_rows_by_head, out_grad, chosen):
    rows, cols = key_vectors.shape
    q_cols = queries.shape[1]
    heads = cols // HEAD_SIZE
    group = q_cols // cols
    local = rows // QB
    chunk = local * KB
    wide = group * rows
    d_model = inputs.shape[1] * tp
    width = d_model // n
    n_chunk = inputs.shape[1] // width
    a = 4
    b = n // a
    units = heads * PARTS
    ucols = group * HEAD_SIZE // PARTS
    blocks = n * rows // KB
    lanes = -(-blocks // 128) * 128
    keys = heads * rows + chunk + (n // 2) * 2 * chunk
    vmem = pl.BlockSpec(memory_space=pltpu.VMEM)
    hbm = pl.BlockSpec(memory_space=pl.ANY)
    dma = pltpu.SemaphoreType.DMA
    outs = (
        ((rows, q_cols), BF16),
        ((rows, cols), BF16),
        ((rows, cols), BF16),
        ((width, q_cols), F32),
    )
    held = pl.pallas_call(
        functools.partial(kernel, n, tp, a, b),
        out_shape=tuple(pltpu.VMEM(s, d) for s, d in outs),
        in_specs=[hbm] * 6,
        out_specs=(vmem,) * 4,
        scratch_shapes=[
            pltpu.VMEM(chosen.shape, jnp.int32),
            pltpu.VMEM((chosen.shape[0], lanes), jnp.int32),
            pltpu.SMEM((chosen.shape[0], lanes), jnp.int32),
            pltpu.VMEM(inputs.shape, BF16),
            pltpu.VMEM((n_chunk, rows, width), BF16),
            pltpu.VMEM((rows, q_cols), BF16),
            pltpu.VMEM((rows, q_cols), BF16),
            pltpu.VMEM((rows, cols), BF16),
            pltpu.VMEM((rows, cols), BF16),
            pltpu.VMEM((heads, wide, 2 * HEAD_SIZE), BF16),
            pltpu.VMEM((heads, wide, 2 * HEAD_SIZE), BF16),
            pltpu.VMEM((heads, rows // KB, KB, 2 * HEAD_SIZE), BF16),
            pltpu.VMEM((heads, n, chunk, 2 * HEAD_SIZE), BF16),
            pltpu.VMEM((heads, n, chunk, 2 * HEAD_SIZE), BF16),
            pltpu.VMEM((a, b, rows, width), BF16),
            pltpu.VMEM((a, b, width, rows), BF16),
            pltpu.VMEM((keys, wide), F32),
            pltpu.VMEM((keys, wide), F32),
            pltpu.VMEM((heads + 1 + n // 2, 1, wide), F32),
            pltpu.VMEM((HEAD_SIZE, wide), F32),
            pltpu.VMEM((heads, n, chunk, 2 * HEAD_SIZE), BF16),
            pltpu.VMEM((heads, n, chunk, 2 * HEAD_SIZE), BF16),
            pltpu.VMEM((heads, rows, 2 * HEAD_SIZE), F32),
            pltpu.VMEM((units, a, rows, ucols), BF16),
            pltpu.VMEM((units, b, width, ucols), BF16),
            pltpu.VMEM((units, b, width, ucols), BF16),
            pltpu.VMEM((units, width, ucols), F32),
            dma((6 + n_chunk,)),
            dma((heads, n)),
            dma((heads, n)),
            dma((n_chunk,)),
            dma((a, b)),
            dma((a, b, tp // 2)),
            dma((heads, n)),
            dma((heads, n)),
            dma((units, a)),
            dma((units, a)),
            dma((units, b)),
            dma((units, b)),
            pltpu.SemaphoreType.REGULAR,
        ],
        compiler_params=pltpu.CompilerParams(
            collective_id=0, has_side_effects=True, vmem_limit_bytes=58 * 1024 * 1024
        ),
    )(chosen, inputs, queries, key_vectors, value_rows_by_head, out_grad)
    return pl.pallas_call(
        write_out,
        out_shape=tuple(jax.ShapeDtypeStruct(s, d) for s, d in outs),
        in_specs=[vmem] * 4,
        out_specs=(hbm,) * 4,
        scratch_shapes=[dma((4,))],
        compiler_params=pltpu.CompilerParams(vmem_limit_bytes=1024 * 1024),
    )(*held)


def solution(mesh):
    n, tp = mesh.shape["kv"], mesh.shape["tp"]
    placed = (P("kv", "tp"),) * 5 + (P(),)
    return jax.shard_map(
        functools.partial(body, n, tp),
        mesh=mesh,
        in_specs=placed,
        out_specs=(P("kv", "tp"),) * 4,
        check_vma=False,
    )
```

```python
import functools

import jax
import jax.numpy as jnp
from jax import lax
from jax.experimental import pallas as pl
from jax.experimental.pallas import tpu as pltpu
from jax.sharding import PartitionSpec as P

HEAD_SIZE = 64
QB = 128
KB = 64
NEG = -1e30
PARTS = 2
BF16 = jnp.bfloat16
F32 = jnp.float32
MESH = pl.DeviceIdType.MESH


def dot_nt(x, y):
    return lax.dot_general(x, y, (((1,), (1,)), ((), ())), preferred_element_type=F32)


def dot_nn(x, y):
    return lax.dot_general(x, y, (((1,), (0,)), ((), ())), preferred_element_type=F32)


def dot_tn(x, y):
    return lax.dot_general(x, y, (((0,), (0,)), ((), ())), preferred_element_type=F32)


def kernel(
    n, tp, a, b,
    chosen_ref, x_ref, q_ref, k_ref, v_ref, g_ref,
    dq_ref, dk_ref, dv_ref, w_ref,
    ch_v, sel_v, sel_s, x_in, xst, q_in, g_in, k_in, v_in, qz, gz, kvown, kvst, kvbuf, xbuf, xt,
    e_buf, dp_buf, mj_buf, dqt, gst, grecv, own_acc, qall, wst, wrecv, w_own,
    ld, kv_send, kv_recv, x_send, x_recv, f_send, g_send, g_recv, q_send, q_recv,
    w_send, w_recv, pair_sem,
):
    me = lax.axis_index("kv")
    t = lax.axis_index("tp")
    alpha = lax.rem(me, a)
    beta = lax.div(me, a)
    parity = lax.rem(t, 2)
    partner = t + 1 - 2 * parity

    def flip(m, step):
        for bit in (1, 2):
            if step & bit:
                m = m + bit - 2 * bit * lax.rem(lax.div(m, bit), 2)
        return m

    rows, cols = k_in.shape
    heads = cols // HEAD_SIZE
    group = q_in.shape[1] // cols
    local = rows // QB
    owner = rows // KB
    chunk = local * KB
    wide = group * rows
    width = xst.shape[2]
    n_chunk = xst.shape[0]
    parts = qall.shape[0] // heads
    ucols = qall.shape[3]
    scale = HEAD_SIZE ** (-0.5)
    single_at = heads * rows
    pair_at = single_at + chunk

    def remote(src, dst, send, recv, kv, tpi):
        return pltpu.make_async_remote_copy(
            src_ref=src, dst_ref=dst, send_sem=send, recv_sem=recv,
            device_id=(kv, tpi), device_id_type=MESH,
        )

    barrier = pltpu.get_barrier_semaphore()
    for d in range(1, n):
        pl.semaphore_signal(
            barrier, inc=1, device_id=(lax.rem(me + d, n), t), device_id_type=MESH
        )
    for d in range(2, tp, 2):
        pl.semaphore_signal(
            barrier, inc=1, device_id=(me, lax.rem(t + d, tp)), device_id_type=MESH
        )
    pl.semaphore_signal(barrier, inc=1, device_id=(me, partner), device_id_type=MESH)

    loads = [
        pltpu.make_async_copy(src, dst, ld.at[i])
        for i, (src, dst) in enumerate(
            [(chosen_ref, ch_v), (k_ref, k_in), (v_ref, v_in), (q_ref, q_in), (g_ref, g_in)]
            + (
                [(x_ref, x_in)]
                if width % 128
                else [
                    (x_ref.at[:, q * width : (q + 1) * width], xst.at[q])
                    for q in range(n_chunk)
                ]
            )
        )
    ]
    for c in loads:
        c.start()

    loads[0].wait()
    picked = ch_v[...]
    ids = lax.broadcasted_iota(jnp.int32, sel_v.shape, 1)
    hit = jnp.zeros(sel_v.shape, jnp.int32)
    for s in range(picked.shape[1]):
        hit = jnp.where(picked[:, s : s + 1] == ids, 1, hit)
    sel_v[...] = hit
    to_scalar = pltpu.make_async_copy(sel_v, sel_s, ld.at[len(loads)])
    to_scalar.start()

    def head_cols(h):
        return slice(h * HEAD_SIZE, (h + 1) * HEAD_SIZE)

    loads[1].wait()
    loads[2].wait()
    for h in range(heads):
        for blk in range(owner):
            at = slice(blk * KB, (blk + 1) * KB)
            kvown[h, blk, :, 0:HEAD_SIZE] = k_in[at, head_cols(h)]
            kvown[h, blk, :, HEAD_SIZE : 2 * HEAD_SIZE] = v_in[at, head_cols(h)]
    to_scalar.wait()

    def used_blocks(i, j):
        used = []
        for blk in range(owner):
            u = sel_s[i * local, j * owner + blk]
            for r in range(1, local):
                u = jnp.maximum(u, sel_s[i * local + r, j * owner + blk])
            used.append(u)
        return used

    def slots(i, j):
        used = used_blocks(i, j)
        picks = []
        for p in range(local):
            before = jnp.int32(0)
            one = []
            for blk in range(owner):
                one.append(jnp.where(before == p, used[blk], 0))
                before = before + used[blk]
            picks.append(one)
        return picks

    def kv_copy(h, i, j):
        return remote(kvst.at[h, i], kvbuf.at[h, j], kv_send.at[h, i], kv_recv.at[h, j], i, t)

    def stage_kv(ii, carry):
        i = n - 1 - ii
        picks = slots(i, me)
        for p in range(local):
            at = jnp.int32(0)
            for blk in range(owner):
                at = at + picks[p][blk] * blk
            for h in range(heads):
                kvst[h, i, p * KB : (p + 1) * KB, :] = kvown[h, at]
        return carry

    lax.fori_loop(0, n - 1 - me, stage_kv, 0)

    pl.semaphore_wait(barrier, n + tp // 2 - 1)

    def send_kv(h):
        def start_kv(ii, carry):
            kv_copy(h, n - 1 - ii, me).start()
            return carry

        lax.fori_loop(0, n - 1 - me, start_kv, 0)

    send_kv(0)

    for c in loads[5:]:
        c.wait()
    if width % 128:
        for q in range(n_chunk):
            xst[q] = x_in[:, q * width : (q + 1) * width]

    def x_copy(q):
        c = t * n_chunk + q
        return remote(
            xst.at[q], xbuf.at[alpha, lax.div(c, a)], x_send.at[q],
            x_recv.at[alpha, lax.div(c, a)], beta * a + lax.rem(c, a), t,
        )

    def send_x(way):
        for q in range(n_chunk):
            c = t * n_chunk + q
            to = lax.rem(c, a)
            rise = lax.div(to, 2) - lax.div(alpha, 2)
            if way < 0:
                due = rise < 0
            elif way > 0:
                due = rise > 0
            else:
                due = jnp.logical_and(rise == 0, to != alpha)

            @pl.when(due)
            def _():
                x_copy(q).start()

            if way == 0:

                @pl.when(to == alpha)
                def _():
                    xbuf[alpha, lax.div(c, a)] = xst[q]

    send_x(-1)

    loads[3].wait()
    loads[4].wait()
    for h in range(heads):
        for gr in range(group):
            hh = h * group + gr
            at = slice(gr * rows, (gr + 1) * rows)
            qz[h, at, 0:HEAD_SIZE] = (q_in[:, head_cols(hh)].astype(F32) * scale).astype(BF16)
            qz[h, at, HEAD_SIZE : 2 * HEAD_SIZE] = jnp.zeros((rows, HEAD_SIZE), BF16)
            gz[h, at, 0:HEAD_SIZE] = jnp.zeros((rows, HEAD_SIZE), BF16)
            gz[h, at, HEAD_SIZE : 2 * HEAD_SIZE] = g_in[:, head_cols(hh)]

    lane = lax.broadcasted_iota(jnp.int32, (1, rows), 1)
    lane_block = lax.div(lane, QB)

    def row_bias(flags):
        vals = [jnp.where(f > 0, F32(0.0), F32(NEG)) for f in flags]
        out = jnp.full((1, rows), vals[0], F32)
        for r in range(1, local):
            out = jnp.where(lane_block == r, vals[r], out)
        return out

    def own_bias():
        return [
            row_bias([sel_s[me * local + r, me * owner + blk] for r in range(local)])
            for blk in range(owner)
        ]

    def far_bias(j):
        picks = slots(me, j)
        out = []
        for p in range(local):
            flags = []
            for r in range(local):
                f = jnp.int32(0)
                for blk in range(owner):
                    f = f + picks[p][blk] * sel_s[me * local + r, j * owner + blk]
                flags.append(f)
            out.append(row_bias(flags))
        return out

    def tile(gr):
        return slice(gr * rows, (gr + 1) * rows)

    def g_copy(h, i, j):
        return remote(gst.at[h, j], grecv.at[h, i], g_send.at[h, j], g_recv.at[h, i], j, t)

    def hop(u):
        return 1 + u % 2

    def q_send_to(h, m, step):
        own = m is alpha
        return remote(
            qall.at[h, m], qall.at[h, m], q_send.at[h, step if own else 0], q_recv.at[h, m],
            beta * a + flip(alpha, step), t,
        )

    def q_here(h, m):
        return remote(qall.at[h, m], qall.at[h, m], q_send.at[h, 0], q_recv.at[h, m], me, t)

    def relay_q(u):
        m = flip(alpha, 3 - hop(u))
        q_here(u, m).wait_recv()
        q_send_to(u, m, hop(u)).start()

    def w_copy(h, bb):
        return remote(
            wst.at[h, bb], wrecv.at[h, beta], w_send.at[h, bb], w_recv.at[h, beta],
            bb * a + alpha, t,
        )

    def first_pass(h, kv, base, idx, bias, causal, stats):
        size = kv.shape[0]
        out = []
        for gr in range(group):
            m, l, rd = stats[gr]
            s = dot_nt(kv, qz[h, tile(gr), :])
            rows_of = []
            for p in range(size // KB):
                part = s[p * KB : (p + 1) * KB] + bias[p]
                if causal:
                    key = p * KB + lax.broadcasted_iota(jnp.int32, (KB, rows), 0)
                    part = jnp.where(key <= lane, part, NEG)
                rows_of.append(part)
            s = jnp.concatenate(rows_of, axis=0)
            mj = jnp.maximum(m, jnp.max(s, axis=0, keepdims=True))
            e = jnp.exp(s - mj)
            dp = dot_nt(kv, gz[h, tile(gr), :])
            e_buf[pl.ds(base, size), tile(gr)] = e
            dp_buf[pl.ds(base, size), tile(gr)] = dp
            mj_buf[idx, :, tile(gr)] = mj
            back = jnp.exp(m - mj)
            l = l * back + jnp.sum(e, axis=0, keepdims=True)
            rd = rd * back + jnp.sum(e * dp, axis=0, keepdims=True)
            out.append((mj, l, rd))
        return tuple(out)

    def second_pass(h, kv, base, idx, stats, first):
        size = kv.shape[0]
        keys = kv[:, 0:HEAD_SIZE]
        out = None
        for gr in range(group):
            m, inv, rd = stats[gr]
            f = jnp.exp(mj_buf[idx, :, tile(gr)] - m) * inv
            p = e_buf[pl.ds(base, size), tile(gr)] * f
            ds = (p * (dp_buf[pl.ds(base, size), tile(gr)] - rd)).astype(BF16)
            term = dot_nn(ds, qz[h, tile(gr), :]) + dot_nn(p.astype(BF16), gz[h, tile(gr), :])
            out = term if out is None else out + term
            dq = dot_tn(keys, ds)
            if first:
                dqt[:, tile(gr)] = dq
            else:
                dqt[:, tile(gr)] += dq
        return out

    odd = lax.rem(me, 2)
    pairs = lax.div(me, 2)

    def own_kv(h):
        return jnp.concatenate([kvown[h, blk] for blk in range(owner)], axis=0)

    def pair_kv(h, jj):
        return jnp.concatenate([kvbuf[h, 2 * jj], kvbuf[h, 2 * jj + 1]], axis=0)

    state = {}

    def own(h):
        none = jnp.full((1, rows), NEG, F32)
        zero = jnp.zeros((1, rows), F32)
        state[h] = first_pass(
            h, own_kv(h), h * rows, h, own_bias(), True, ((none, zero, zero),) * group
        )

    def far(h):
        def one_single(_, stats):
            j = me - 1
            kv_copy(h, j, j).wait_recv()
            return first_pass(h, kvbuf[h, j], single_at, heads, far_bias(j), False, stats)

        stats = state[h]
        stats = lax.fori_loop(0, odd, one_single, stats)

        def one_pair(ii, stats):
            jj = pairs - 1 - ii
            for d in range(2):
                kv_copy(h, 2 * jj + d, 2 * jj + d).wait_recv()
            base = pl.multiple_of(pair_at + jj * (2 * chunk), chunk)
            bias = far_bias(2 * jj) + far_bias(2 * jj + 1)
            return first_pass(h, pair_kv(h, jj), base, heads + 1 + jj, bias, False, stats)

        stats = lax.fori_loop(0, pairs, one_pair, stats)
        fin = []
        for m, l, rd in stats:
            inv = 1.0 / l
            fin.append((m, inv, rd * inv))
        state[h] = fin

    def back(h):
        fin = state[h]
        dqt[...] = jnp.zeros_like(dqt)

        def back_pair(jj, carry):
            base = pl.multiple_of(pair_at + jj * (2 * chunk), chunk)
            out = second_pass(h, pair_kv(h, jj), base, heads + 1 + jj, fin, False).astype(BF16)
            for d in range(2):
                gst[h, 2 * jj + d] = out[d * chunk : (d + 1) * chunk]
            for d in range(2):
                g_copy(h, me, 2 * jj + d).start()
            return carry

        lax.fori_loop(0, pairs, back_pair, 0)

        def back_single(_, carry):
            j = me - 1
            gst[h, j] = second_pass(h, kvbuf[h, j], single_at, heads, fin, False).astype(BF16)
            g_copy(h, me, j).start()
            return carry

        lax.fori_loop(0, odd, back_single, 0)
        own_acc[h] = second_pass(h, own_kv(h), h * rows, h, fin, False)

        per = group // parts
        for u in range(parts):
            stacked = jnp.concatenate(
                [dqt[:, tile(gr)] for gr in range(u * per, (u + 1) * per)], axis=0
            )
            part = (stacked * scale).T.astype(BF16)
            at = h * parts + u
            qall[at, alpha] = part
            dq_ref[:, at * ucols : (at + 1) * ucols] = part
            for step in (2, 1):
                q_send_to(at, alpha, step).start()

    def send_g(h):
        def start_g(j, carry):
            g_copy(h, me, j).start()
            return carry

        lax.fori_loop(0, me, start_g, 0)

    def x_source(bb):
        return lax.div(bb * a + alpha, n_chunk)

    def x_here(m, bb):
        return remote(xst.at[0], xbuf.at[m, bb], x_send.at[0], x_recv.at[m, bb], me, t)

    def x_forward(m, bb, d):
        to = partner if d == 0 else lax.rem(t + 2 * d, tp)
        return remote(
            xbuf.at[m, bb], xbuf.at[m, bb], f_send.at[m, bb, d], x_recv.at[m, bb], me, to
        )

    def relay_x(step):
        m = flip(alpha, step)
        for bb in range(b):

            @pl.when(x_source(bb) == t)
            def _():
                if step:
                    x_here(m, bb).wait_recv()
                for d in range(tp // 2 - 1, -1, -1):
                    x_forward(m, bb, d).start()

    def relay_far(early):
        lower = lax.rem(lax.div(alpha, 2), 2) == 0

        @pl.when(lower if early else jnp.logical_not(lower))
        def _():
            relay_x(2)
            relay_x(3)

    def gather_x():
        for step in range(a):
            m = flip(alpha, step)
            for bb in range(b):
                src = x_source(bb)

                @pl.when(src != t)
                def _():
                    x_here(m, bb).wait_recv()

                @pl.when(jnp.logical_and(src != t, lax.rem(src, 2) == parity))
                def _():
                    x_forward(m, bb, 0).start()

        for bb in range(b):
            for m in range(a):
                xt[m, bb] = xbuf[m, bb].T

    def weight_part(h):
        q_here(h, flip(alpha, hop(h))).wait_recv()
        q_here(h, flip(alpha, 3)).wait_recv()

        def partial(bb):
            out = dot_nn(xt[0, bb], qall[h, 0])
            for m in range(1, a):
                out = out + dot_nn(xt[m, bb], qall[h, m])
            return out

        for d in range(1, b):
            bb = lax.rem(beta + d, b)
            wst[h, bb] = partial(bb).astype(BF16)
            w_copy(h, bb).start()
        w_own[h] = partial(beta)

    def wait_kv(h):
        def done_kv(i, carry):
            kv_copy(h, i, me).wait_send()
            return carry

        lax.fori_loop(me + 1, n, done_kv, 0)

    own(0)
    wait_kv(0)
    pl.semaphore_signal(pair_sem, inc=1, device_id=(me, partner), device_id_type=MESH)
    if heads > 1:
        own(1)
    pl.semaphore_wait(pair_sem, 1)
    for h in range(1, heads):
        send_kv(h)
    send_x(0)
    far(0)
    back(0)
    send_x(1)
    relay_x(0)
    relay_x(1)
    relay_far(True)
    for h in range(1, heads):
        if h > 1:
            own(h)
        far(h)
        for u in range((h - 1) * parts, h * parts):
            relay_q(u)
        back(h)
    relay_far(False)
    gather_x()
    last = (heads - 1) * parts
    for u in range(last):
        weight_part(u)
    for u in range(last, heads * parts):
        relay_q(u)
    for u in range(last, heads * parts):
        weight_part(u)

    for h in range(heads):

        def add_far(i, carry):
            remote(gst.at[h, 0], grecv.at[h, i], g_send.at[h, 0], g_recv.at[h, i], me, t).wait_recv()
            picks = slots(i, me)
            for p in range(local):
                got = grecv[h, i, p * KB : (p + 1) * KB, :].astype(F32)
                for blk in range(owner):
                    own_acc[h, blk * KB : (blk + 1) * KB, :] += jnp.where(
                        picks[p][blk] > 0, got, 0.0
                    )
            return carry

        lax.fori_loop(me + 1, n, add_far, 0)
        dk_ref[:, head_cols(h)] = own_acc[h, :, 0:HEAD_SIZE].astype(BF16)
        dv_ref[:, head_cols(h)] = own_acc[h, :, HEAD_SIZE : 2 * HEAD_SIZE].astype(BF16)

    def wait_w(h):
        total = w_own[h]
        for d in range(1, b):
            bb = lax.rem(beta + d, b)
            remote(
                wst.at[h, bb], wrecv.at[h, bb], w_send.at[h, bb], w_recv.at[h, bb], me, t
            ).wait_recv()
            total = total + wrecv[h, bb].astype(F32)
        w_ref[:, h * ucols : (h + 1) * ucols] = total

    for h in range(heads * parts):
        wait_w(h)

    for h in range(1, heads):
        wait_kv(h)
    for q in range(n_chunk):

        @pl.when(lax.rem(t * n_chunk + q, a) != alpha)
        def _():
            x_copy(q).wait_send()

    for bb in range(b):
        src = x_source(bb)
        for m in range(a):

            @pl.when(lax.rem(src, 2) == parity)
            def _():
                x_forward(m, bb, 0).wait_send()

            @pl.when(src == t)
            def _():
                for d in range(1, tp // 2):
                    x_forward(m, bb, d).wait_send()

    for h in range(heads):

        def done_g(j, carry):
            g_copy(h, me, j).wait_send()
            return carry

        lax.fori_loop(0, me, done_g, 0)

    for u in range(heads * parts):
        for step in (2, 1):
            q_send_to(u, alpha, step).wait_send()
        q_send_to(u, flip(alpha, 3 - hop(u)), hop(u)).wait_send()
        for d in range(1, b):
            w_copy(u, lax.rem(beta + d, b)).wait_send()


def write_out(*refs):
    count = (len(refs) - 1) // 2
    sems = refs[-1]
    copies = [
        pltpu.make_async_copy(refs[i], refs[count + i], sems.at[i]) for i in range(count)
    ]
    for c in copies:
        c.start()
    for c in copies:
        c.wait()


def body(n, tp, inputs, queries, key_vectors, value_rows_by_head, out_grad, chosen):
    rows, cols = key_vectors.shape
    q_cols = queries.shape[1]
    heads = cols // HEAD_SIZE
    group = q_cols // cols
    local = rows // QB
    chunk = local * KB
    wide = group * rows
    d_model = inputs.shape[1] * tp
    width = d_model // n
    n_chunk = inputs.shape[1] // width
    a = 4
    b = n // a
    units = heads * PARTS
    ucols = group * HEAD_SIZE // PARTS
    blocks = n * rows // KB
    lanes = -(-blocks // 128) * 128
    keys = heads * rows + chunk + (n // 2) * 2 * chunk
    vmem = pl.BlockSpec(memory_space=pltpu.VMEM)
    hbm = pl.BlockSpec(memory_space=pl.ANY)
    dma = pltpu.SemaphoreType.DMA
    outs = (
        ((rows, q_cols), BF16),
        ((rows, cols), BF16),
        ((rows, cols), BF16),
        ((width, q_cols), F32),
    )
    held = pl.pallas_call(
        functools.partial(kernel, n, tp, a, b),
        out_shape=tuple(pltpu.VMEM(s, d) for s, d in outs),
        in_specs=[hbm] * 6,
        out_specs=(vmem,) * 4,
        scratch_shapes=[
            pltpu.VMEM(chosen.shape, jnp.int32),
            pltpu.VMEM((chosen.shape[0], lanes), jnp.int32),
            pltpu.SMEM((chosen.shape[0], lanes), jnp.int32),
            pltpu.VMEM(inputs.shape, BF16),
            pltpu.VMEM((n_chunk, rows, width), BF16),
            pltpu.VMEM((rows, q_cols), BF16),
            pltpu.VMEM((rows, q_cols), BF16),
            pltpu.VMEM((rows, cols), BF16),
            pltpu.VMEM((rows, cols), BF16),
            pltpu.VMEM((heads, wide, 2 * HEAD_SIZE), BF16),
            pltpu.VMEM((heads, wide, 2 * HEAD_SIZE), BF16),
            pltpu.VMEM((heads, rows // KB, KB, 2 * HEAD_SIZE), BF16),
            pltpu.VMEM((heads, n, chunk, 2 * HEAD_SIZE), BF16),
            pltpu.VMEM((heads, n, chunk, 2 * HEAD_SIZE), BF16),
            pltpu.VMEM((a, b, rows, width), BF16),
            pltpu.VMEM((a, b, width, rows), BF16),
            pltpu.VMEM((keys, wide), F32),
            pltpu.VMEM((keys, wide), F32),
            pltpu.VMEM((heads + 1 + n // 2, 1, wide), F32),
            pltpu.VMEM((HEAD_SIZE, wide), F32),
            pltpu.VMEM((heads, n, chunk, 2 * HEAD_SIZE), BF16),
            pltpu.VMEM((heads, n, chunk, 2 * HEAD_SIZE), BF16),
            pltpu.VMEM((heads, rows, 2 * HEAD_SIZE), F32),
            pltpu.VMEM((units, a, rows, ucols), BF16),
            pltpu.VMEM((units, b, width, ucols), BF16),
            pltpu.VMEM((units, b, width, ucols), BF16),
            pltpu.VMEM((units, width, ucols), F32),
            dma((6 + n_chunk,)),
            dma((heads, n)),
            dma((heads, n)),
            dma((n_chunk,)),
            dma((a, b)),
            dma((a, b, tp // 2)),
            dma((heads, n)),
            dma((heads, n)),
            dma((units, a)),
            dma((units, a)),
            dma((units, b)),
            dma((units, b)),
            pltpu.SemaphoreType.REGULAR,
        ],
        compiler_params=pltpu.CompilerParams(
            collective_id=0, has_side_effects=True, vmem_limit_bytes=58 * 1024 * 1024
        ),
    )(chosen, inputs, queries, key_vectors, value_rows_by_head, out_grad)
    return pl.pallas_call(
        write_out,
        out_shape=tuple(jax.ShapeDtypeStruct(s, d) for s, d in outs),
        in_specs=[vmem] * 4,
        out_specs=(hbm,) * 4,
        scratch_shapes=[dma((4,))],
        compiler_params=pltpu.CompilerParams(vmem_limit_bytes=1024 * 1024),
    )(*held)


def solution(mesh):
    n, tp = mesh.shape["kv"], mesh.shape["tp"]
    placed = (P("kv", "tp"),) * 5 + (P(),)
    return jax.shard_map(
        functools.partial(body, n, tp),
        mesh=mesh,
        in_specs=placed,
        out_specs=(P("kv", "tp"),) * 4,
        check_vma=False,
    )
```

```python
import functools

import jax
import jax.numpy as jnp
from jax import lax
from jax.experimental import pallas as pl
from jax.experimental.pallas import tpu as pltpu
from jax.sharding import PartitionSpec as P

HEAD_SIZE = 64
QB = 128
KB = 64
NEG = -1e30
PARTS = 2
BF16 = jnp.bfloat16
F32 = jnp.float32
MESH = pl.DeviceIdType.MESH


def dot_nt(x, y):
    return lax.dot_general(x, y, (((1,), (1,)), ((), ())), preferred_element_type=F32)


def dot_nn(x, y):
    return lax.dot_general(x, y, (((1,), (0,)), ((), ())), preferred_element_type=F32)


def dot_tn(x, y):
    return lax.dot_general(x, y, (((0,), (0,)), ((), ())), preferred_element_type=F32)


def kernel(
    n, tp, a, b,
    chosen_ref, x_ref, q_ref, k_ref, v_ref, g_ref,
    dq_ref, dk_ref, dv_ref, w_ref,
    ch_v, sel_v, sel_s, x_in, xst, q_in, g_in, k_in, v_in, qz, gz, kvown, kvst, kvbuf, xbuf, xt,
    e_buf, dp_buf, mj_buf, dqt, gst, grecv, own_acc, qall, wst, wrecv, w_own,
    ld, kv_send, kv_recv, x_send, x_recv, f_send, g_send, g_recv, q_send, q_recv,
    w_send, w_recv, pair_sem,
):
    me = lax.axis_index("kv")
    t = lax.axis_index("tp")
    alpha = lax.rem(me, a)
    beta = lax.div(me, a)
    parity = lax.rem(t, 2)
    partner = t + 1 - 2 * parity

    def flip(m, step):
        for bit in (1, 2):
            if step & bit:
                m = m + bit - 2 * bit * lax.rem(lax.div(m, bit), 2)
        return m

    rows, cols = k_in.shape
    heads = cols // HEAD_SIZE
    group = q_in.shape[1] // cols
    local = rows // QB
    owner = rows // KB
    chunk = local * KB
    wide = group * rows
    width = xst.shape[2]
    n_chunk = xst.shape[0]
    parts = qall.shape[0] // heads
    ucols = qall.shape[3]
    scale = HEAD_SIZE ** (-0.5)
    single_at = heads * rows
    pair_at = single_at + chunk

    def remote(src, dst, send, recv, kv, tpi):
        return pltpu.make_async_remote_copy(
            src_ref=src, dst_ref=dst, send_sem=send, recv_sem=recv,
            device_id=(kv, tpi), device_id_type=MESH,
        )

    barrier = pltpu.get_barrier_semaphore()
    for d in range(1, n):
        pl.semaphore_signal(
            barrier, inc=1, device_id=(lax.rem(me + d, n), t), device_id_type=MESH
        )
    for d in range(2, tp, 2):
        pl.semaphore_signal(
            barrier, inc=1, device_id=(me, lax.rem(t + d, tp)), device_id_type=MESH
        )
    pl.semaphore_signal(barrier, inc=1, device_id=(me, partner), device_id_type=MESH)

    loads = [
        pltpu.make_async_copy(src, dst, ld.at[i])
        for i, (src, dst) in enumerate(
            [(chosen_ref, ch_v), (k_ref, k_in), (v_ref, v_in), (q_ref, q_in), (g_ref, g_in)]
            + (
                [(x_ref, x_in)]
                if width % 128
                else [
                    (x_ref.at[:, q * width : (q + 1) * width], xst.at[q])
                    for q in range(n_chunk)
                ]
            )
        )
    ]
    for c in loads:
        c.start()

    loads[0].wait()
    picked = ch_v[...]
    ids = lax.broadcasted_iota(jnp.int32, sel_v.shape, 1)
    hit = jnp.zeros(sel_v.shape, jnp.int32)
    for s in range(picked.shape[1]):
        hit = jnp.where(picked[:, s : s + 1] == ids, 1, hit)
    sel_v[...] = hit
    to_scalar = pltpu.make_async_copy(sel_v, sel_s, ld.at[len(loads)])
    to_scalar.start()

    def head_cols(h):
        return slice(h * HEAD_SIZE, (h + 1) * HEAD_SIZE)

    loads[1].wait()
    loads[2].wait()
    for h in range(heads):
        for blk in range(owner):
            at = slice(blk * KB, (blk + 1) * KB)
            kvown[h, blk, :, 0:HEAD_SIZE] = k_in[at, head_cols(h)]
            kvown[h, blk, :, HEAD_SIZE : 2 * HEAD_SIZE] = v_in[at, head_cols(h)]
    to_scalar.wait()

    def used_blocks(i, j):
        used = []
        for blk in range(owner):
            u = sel_s[i * local, j * owner + blk]
            for r in range(1, local):
                u = jnp.maximum(u, sel_s[i * local + r, j * owner + blk])
            used.append(u)
        return used

    def slots(i, j):
        used = used_blocks(i, j)
        picks = []
        for p in range(local):
            before = jnp.int32(0)
            one = []
            for blk in range(owner):
                one.append(jnp.where(before == p, used[blk], 0))
                before = before + used[blk]
            picks.append(one)
        return picks

    def kv_copy(h, i, j):
        return remote(kvst.at[h, i], kvbuf.at[h, j], kv_send.at[h, i], kv_recv.at[h, j], i, t)

    def stage_kv(ii, carry):
        i = n - 1 - ii
        picks = slots(i, me)
        for p in range(local):
            at = jnp.int32(0)
            for blk in range(owner):
                at = at + picks[p][blk] * blk
            for h in range(heads):
                kvst[h, i, p * KB : (p + 1) * KB, :] = kvown[h, at]
        return carry

    lax.fori_loop(0, n - 1 - me, stage_kv, 0)

    pl.semaphore_wait(barrier, n + tp // 2 - 1)

    def send_kv(h):
        def start_kv(ii, carry):
            kv_copy(h, n - 1 - ii, me).start()
            return carry

        lax.fori_loop(0, n - 1 - me, start_kv, 0)

    send_kv(0)

    for c in loads[5:]:
        c.wait()
    if width % 128:
        for q in range(n_chunk):
            xst[q] = x_in[:, q * width : (q + 1) * width]

    def x_copy(q):
        c = t * n_chunk + q
        return remote(
            xst.at[q], xbuf.at[alpha, lax.div(c, a)], x_send.at[q],
            x_recv.at[alpha, lax.div(c, a)], beta * a + lax.rem(c, a), t,
        )

    def send_x(way):
        for q in range(n_chunk):
            c = t * n_chunk + q
            to = lax.rem(c, a)
            rise = lax.div(to, 2) - lax.div(alpha, 2)
            if way < 0:
                due = rise < 0
            elif way > 0:
                due = rise > 0
            else:
                due = jnp.logical_and(rise == 0, to != alpha)

            @pl.when(due)
            def _():
                x_copy(q).start()

            if way == 0:

                @pl.when(to == alpha)
                def _():
                    xbuf[alpha, lax.div(c, a)] = xst[q]

    send_x(-1)

    loads[3].wait()
    loads[4].wait()
    for h in range(heads):
        for gr in range(group):
            hh = h * group + gr
            at = slice(gr * rows, (gr + 1) * rows)
            qz[h, at, 0:HEAD_SIZE] = (q_in[:, head_cols(hh)].astype(F32) * scale).astype(BF16)
            qz[h, at, HEAD_SIZE : 2 * HEAD_SIZE] = jnp.zeros((rows, HEAD_SIZE), BF16)
            gz[h, at, 0:HEAD_SIZE] = jnp.zeros((rows, HEAD_SIZE), BF16)
            gz[h, at, HEAD_SIZE : 2 * HEAD_SIZE] = g_in[:, head_cols(hh)]

    lane = lax.broadcasted_iota(jnp.int32, (1, rows), 1)
    lane_block = lax.div(lane, QB)

    def row_bias(flags):
        vals = [jnp.where(f > 0, F32(0.0), F32(NEG)) for f in flags]
        out = jnp.full((1, rows), vals[0], F32)
        for r in range(1, local):
            out = jnp.where(lane_block == r, vals[r], out)
        return out

    def own_bias():
        return [
            row_bias([sel_s[me * local + r, me * owner + blk] for r in range(local)])
            for blk in range(owner)
        ]

    def far_bias(j):
        picks = slots(me, j)
        out = []
        for p in range(local):
            flags = []
            for r in range(local):
                f = jnp.int32(0)
                for blk in range(owner):
                    f = f + picks[p][blk] * sel_s[me * local + r, j * owner + blk]
                flags.append(f)
            out.append(row_bias(flags))
        return out

    def tile(gr):
        return slice(gr * rows, (gr + 1) * rows)

    def g_copy(h, i, j):
        return remote(gst.at[h, j], grecv.at[h, i], g_send.at[h, j], g_recv.at[h, i], j, t)

    def hop(u):
        return 1 + u % 2

    def q_send_to(h, m, step):
        own = m is alpha
        return remote(
            qall.at[h, m], qall.at[h, m], q_send.at[h, step if own else 0], q_recv.at[h, m],
            beta * a + flip(alpha, step), t,
        )

    def q_here(h, m):
        return remote(qall.at[h, m], qall.at[h, m], q_send.at[h, 0], q_recv.at[h, m], me, t)

    def relay_q(u):
        m = flip(alpha, 3 - hop(u))
        q_here(u, m).wait_recv()
        q_send_to(u, m, hop(u)).start()

    def w_copy(h, bb):
        return remote(
            wst.at[h, bb], wrecv.at[h, beta], w_send.at[h, bb], w_recv.at[h, beta],
            bb * a + alpha, t,
        )

    def first_pass(h, kv, base, idx, bias, causal, stats):
        size = kv.shape[0]
        out = []
        for gr in range(group):
            m, l, rd = stats[gr]
            s = dot_nt(kv, qz[h, tile(gr), :])
            rows_of = []
            for p in range(size // KB):
                part = s[p * KB : (p + 1) * KB] + bias[p]
                if causal:
                    key = p * KB + lax.broadcasted_iota(jnp.int32, (KB, rows), 0)
                    part = jnp.where(key <= lane, part, NEG)
                rows_of.append(part)
            s = jnp.concatenate(rows_of, axis=0)
            mj = jnp.maximum(m, jnp.max(s, axis=0, keepdims=True))
            e = jnp.exp(s - mj)
            dp = dot_nt(kv, gz[h, tile(gr), :])
            e_buf[pl.ds(base, size), tile(gr)] = e
            dp_buf[pl.ds(base, size), tile(gr)] = dp
            mj_buf[idx, :, tile(gr)] = mj
            back = jnp.exp(m - mj)
            l = l * back + jnp.sum(e, axis=0, keepdims=True)
            rd = rd * back + jnp.sum(e * dp, axis=0, keepdims=True)
            out.append((mj, l, rd))
        return tuple(out)

    def second_pass(h, kv, base, idx, stats, first):
        size = kv.shape[0]
        keys = kv[:, 0:HEAD_SIZE]
        out = None
        for gr in range(group):
            m, inv, rd = stats[gr]
            f = jnp.exp(mj_buf[idx, :, tile(gr)] - m) * inv
            p = e_buf[pl.ds(base, size), tile(gr)] * f
            ds = (p * (dp_buf[pl.ds(base, size), tile(gr)] - rd)).astype(BF16)
            term = dot_nn(ds, qz[h, tile(gr), :]) + dot_nn(p.astype(BF16), gz[h, tile(gr), :])
            out = term if out is None else out + term
            dq = dot_tn(keys, ds)
            if first:
                dqt[:, tile(gr)] = dq
            else:
                dqt[:, tile(gr)] += dq
        return out

    odd = lax.rem(me, 2)
    pairs = lax.div(me, 2)

    def own_kv(h):
        return jnp.concatenate([kvown[h, blk] for blk in range(owner)], axis=0)

    def pair_kv(h, jj):
        return jnp.concatenate([kvbuf[h, 2 * jj], kvbuf[h, 2 * jj + 1]], axis=0)

    state = {}

    def own(h):
        none = jnp.full((1, rows), NEG, F32)
        zero = jnp.zeros((1, rows), F32)
        state[h] = first_pass(
            h, own_kv(h), h * rows, h, own_bias(), True, ((none, zero, zero),) * group
        )

    def far(h):
        def one_single(_, stats):
            j = me - 1
            kv_copy(h, j, j).wait_recv()
            return first_pass(h, kvbuf[h, j], single_at, heads, far_bias(j), False, stats)

        stats = state[h]
        stats = lax.fori_loop(0, odd, one_single, stats)

        def one_pair(ii, stats):
            jj = pairs - 1 - ii
            for d in range(2):
                kv_copy(h, 2 * jj + d, 2 * jj + d).wait_recv()
            base = pl.multiple_of(pair_at + jj * (2 * chunk), chunk)
            bias = far_bias(2 * jj) + far_bias(2 * jj + 1)
            return first_pass(h, pair_kv(h, jj), base, heads + 1 + jj, bias, False, stats)

        stats = lax.fori_loop(0, pairs, one_pair, stats)
        fin = []
        for m, l, rd in stats:
            inv = 1.0 / l
            fin.append((m, inv, rd * inv))
        state[h] = fin

    def back(h):
        fin = state[h]
        dqt[...] = jnp.zeros_like(dqt)

        def back_pair(jj, carry):
            base = pl.multiple_of(pair_at + jj * (2 * chunk), chunk)
            out = second_pass(h, pair_kv(h, jj), base, heads + 1 + jj, fin, False).astype(BF16)
            for d in range(2):
                gst[h, 2 * jj + d] = out[d * chunk : (d + 1) * chunk]
            for d in range(2):
                g_copy(h, me, 2 * jj + d).start()
            return carry

        lax.fori_loop(0, pairs, back_pair, 0)

        def back_single(_, carry):
            j = me - 1
            gst[h, j] = second_pass(h, kvbuf[h, j], single_at, heads, fin, False).astype(BF16)
            g_copy(h, me, j).start()
            return carry

        lax.fori_loop(0, odd, back_single, 0)
        own_acc[h] = second_pass(h, own_kv(h), h * rows, h, fin, False)

        per = group // parts
        for u in range(parts):
            stacked = jnp.concatenate(
                [dqt[:, tile(gr)] for gr in range(u * per, (u + 1) * per)], axis=0
            )
            part = (stacked * scale).T.astype(BF16)
            at = h * parts + u
            qall[at, alpha] = part
            dq_ref[:, at * ucols : (at + 1) * ucols] = part
            for step in (1, 2):
                q_send_to(at, alpha, step).start()

    def send_g(h):
        def start_g(j, carry):
            g_copy(h, me, j).start()
            return carry

        lax.fori_loop(0, me, start_g, 0)

    def x_source(bb):
        return lax.div(bb * a + alpha, n_chunk)

    def x_here(m, bb):
        return remote(xst.at[0], xbuf.at[m, bb], x_send.at[0], x_recv.at[m, bb], me, t)

    def x_forward(m, bb, d):
        to = partner if d == 0 else lax.rem(t + 2 * d, tp)
        return remote(
            xbuf.at[m, bb], xbuf.at[m, bb], f_send.at[m, bb, d], x_recv.at[m, bb], me, to
        )

    def relay_x(step):
        m = flip(alpha, step)
        for bb in range(b):

            @pl.when(x_source(bb) == t)
            def _():
                if step:
                    x_here(m, bb).wait_recv()
                for d in range(tp // 2 - 1, -1, -1):
                    x_forward(m, bb, d).start()

    def relay_far(early):
        lower = lax.rem(lax.div(alpha, 2), 2) == 0

        @pl.when(lower if early else jnp.logical_not(lower))
        def _():
            relay_x(2)
            relay_x(3)

    def gather_x():
        for step in range(a):
            m = flip(alpha, step)
            for bb in range(b):
                src = x_source(bb)

                @pl.when(src != t)
                def _():
                    x_here(m, bb).wait_recv()

                @pl.when(jnp.logical_and(src != t, lax.rem(src, 2) == parity))
                def _():
                    x_forward(m, bb, 0).start()

        for bb in range(b):
            for m in range(a):
                xt[m, bb] = xbuf[m, bb].T

    def weight_part(h):
        q_here(h, flip(alpha, hop(h))).wait_recv()
        q_here(h, flip(alpha, 3)).wait_recv()

        def partial(bb):
            out = dot_nn(xt[0, bb], qall[h, 0])
            for m in range(1, a):
                out = out + dot_nn(xt[m, bb], qall[h, m])
            return out

        for d in range(1, b):
            bb = lax.rem(beta + d, b)
            wst[h, bb] = partial(bb).astype(BF16)
            w_copy(h, bb).start()

    def wait_kv(h):
        def done_kv(i, carry):
            kv_copy(h, i, me).wait_send()
            return carry

        lax.fori_loop(me + 1, n, done_kv, 0)

    own(0)
    wait_kv(0)
    pl.semaphore_signal(pair_sem, inc=1, device_id=(me, partner), device_id_type=MESH)
    if heads > 1:
        own(1)
    pl.semaphore_wait(pair_sem, 1)
    for h in range(1, heads):
        send_kv(h)
    send_x(0)
    far(0)
    back(0)
    relay_x(0)
    send_x(1)
    relay_x(1)
    relay_far(True)
    for h in range(1, heads):
        if h > 1:
            own(h)
        far(h)
        for u in range((h - 1) * parts, h * parts):
            relay_q(u)
        back(h)
    relay_far(False)
    gather_x()
    last = (heads - 1) * parts
    for u in range(last):
        weight_part(u)
    for u in range(last, heads * parts):
        relay_q(u)
    for u in range(last, heads * parts):
        weight_part(u)

    def own_part(h, bb):
        out = dot_nn(xt[0, bb], qall[h, 0])
        for m in range(1, a):
            out = out + dot_nn(xt[m, bb], qall[h, m])
        return out

    for h in range(heads * parts):
        w_own[h] = own_part(h, beta)

    for h in range(heads):

        def add_far(i, carry):
            remote(gst.at[h, 0], grecv.at[h, i], g_send.at[h, 0], g_recv.at[h, i], me, t).wait_recv()
            picks = slots(i, me)
            for p in range(local):
                got = grecv[h, i, p * KB : (p + 1) * KB, :].astype(F32)
                for blk in range(owner):
                    own_acc[h, blk * KB : (blk + 1) * KB, :] += jnp.where(
                        picks[p][blk] > 0, got, 0.0
                    )
            return carry

        lax.fori_loop(me + 1, n, add_far, 0)
        dk_ref[:, head_cols(h)] = own_acc[h, :, 0:HEAD_SIZE].astype(BF16)
        dv_ref[:, head_cols(h)] = own_acc[h, :, HEAD_SIZE : 2 * HEAD_SIZE].astype(BF16)

    def wait_w(h):
        total = w_own[h]
        for d in range(1, b):
            bb = lax.rem(beta + d, b)
            remote(
                wst.at[h, bb], wrecv.at[h, bb], w_send.at[h, bb], w_recv.at[h, bb], me, t
            ).wait_recv()
            total = total + wrecv[h, bb].astype(F32)
        w_ref[:, h * ucols : (h + 1) * ucols] = total

    for h in range(heads * parts):
        wait_w(h)

    for h in range(1, heads):
        wait_kv(h)
    for q in range(n_chunk):

        @pl.when(lax.rem(t * n_chunk + q, a) != alpha)
        def _():
            x_copy(q).wait_send()

    for bb in range(b):
        src = x_source(bb)
        for m in range(a):

            @pl.when(lax.rem(src, 2) == parity)
            def _():
                x_forward(m, bb, 0).wait_send()

            @pl.when(src == t)
            def _():
                for d in range(1, tp // 2):
                    x_forward(m, bb, d).wait_send()

    for h in range(heads):

        def done_g(j, carry):
            g_copy(h, me, j).wait_send()
            return carry

        lax.fori_loop(0, me, done_g, 0)

    for u in range(heads * parts):
        for step in (2, 1):
            q_send_to(u, alpha, step).wait_send()
        q_send_to(u, flip(alpha, 3 - hop(u)), hop(u)).wait_send()
        for d in range(1, b):
            w_copy(u, lax.rem(beta + d, b)).wait_send()


def write_out(*refs):
    count = (len(refs) - 1) // 2
    sems = refs[-1]
    copies = [
        pltpu.make_async_copy(refs[i], refs[count + i], sems.at[i]) for i in range(count)
    ]
    for c in copies:
        c.start()
    for c in copies:
        c.wait()


def body(n, tp, inputs, queries, key_vectors, value_rows_by_head, out_grad, chosen):
    rows, cols = key_vectors.shape
    q_cols = queries.shape[1]
    heads = cols // HEAD_SIZE
    group = q_cols // cols
    local = rows // QB
    chunk = local * KB
    wide = group * rows
    d_model = inputs.shape[1] * tp
    width = d_model // n
    n_chunk = inputs.shape[1] // width
    a = 4
    b = n // a
    units = heads * PARTS
    ucols = group * HEAD_SIZE // PARTS
    blocks = n * rows // KB
    lanes = -(-blocks // 128) * 128
    keys = heads * rows + chunk + (n // 2) * 2 * chunk
    vmem = pl.BlockSpec(memory_space=pltpu.VMEM)
    hbm = pl.BlockSpec(memory_space=pl.ANY)
    dma = pltpu.SemaphoreType.DMA
    outs = (
        ((rows, q_cols), BF16),
        ((rows, cols), BF16),
        ((rows, cols), BF16),
        ((width, q_cols), F32),
    )
    held = pl.pallas_call(
        functools.partial(kernel, n, tp, a, b),
        out_shape=tuple(pltpu.VMEM(s, d) for s, d in outs),
        in_specs=[hbm] * 6,
        out_specs=(vmem,) * 4,
        scratch_shapes=[
            pltpu.VMEM(chosen.shape, jnp.int32),
            pltpu.VMEM((chosen.shape[0], lanes), jnp.int32),
            pltpu.SMEM((chosen.shape[0], lanes), jnp.int32),
            pltpu.VMEM(inputs.shape, BF16),
            pltpu.VMEM((n_chunk, rows, width), BF16),
            pltpu.VMEM((rows, q_cols), BF16),
            pltpu.VMEM((rows, q_cols), BF16),
            pltpu.VMEM((rows, cols), BF16),
            pltpu.VMEM((rows, cols), BF16),
            pltpu.VMEM((heads, wide, 2 * HEAD_SIZE), BF16),
            pltpu.VMEM((heads, wide, 2 * HEAD_SIZE), BF16),
            pltpu.VMEM((heads, rows // KB, KB, 2 * HEAD_SIZE), BF16),
            pltpu.VMEM((heads, n, chunk, 2 * HEAD_SIZE), BF16),
            pltpu.VMEM((heads, n, chunk, 2 * HEAD_SIZE), BF16),
            pltpu.VMEM((a, b, rows, width), BF16),
            pltpu.VMEM((a, b, width, rows), BF16),
            pltpu.VMEM((keys, wide), F32),
            pltpu.VMEM((keys, wide), F32),
            pltpu.VMEM((heads + 1 + n // 2, 1, wide), F32),
            pltpu.VMEM((HEAD_SIZE, wide), F32),
            pltpu.VMEM((heads, n, chunk, 2 * HEAD_SIZE), BF16),
            pltpu.VMEM((heads, n, chunk, 2 * HEAD_SIZE), BF16),
            pltpu.VMEM((heads, rows, 2 * HEAD_SIZE), F32),
            pltpu.VMEM((units, a, rows, ucols), BF16),
            pltpu.VMEM((units, b, width, ucols), BF16),
            pltpu.VMEM((units, b, width, ucols), BF16),
            pltpu.VMEM((units, width, ucols), F32),
            dma((6 + n_chunk,)),
            dma((heads, n)),
            dma((heads, n)),
            dma((n_chunk,)),
            dma((a, b)),
            dma((a, b, tp // 2)),
            dma((heads, n)),
            dma((heads, n)),
            dma((units, a)),
            dma((units, a)),
            dma((units, b)),
            dma((units, b)),
            pltpu.SemaphoreType.REGULAR,
        ],
        compiler_params=pltpu.CompilerParams(
            collective_id=0, has_side_effects=True, vmem_limit_bytes=58 * 1024 * 1024
        ),
    )(chosen, inputs, queries, key_vectors, value_rows_by_head, out_grad)
    return pl.pallas_call(
        write_out,
        out_shape=tuple(jax.ShapeDtypeStruct(s, d) for s, d in outs),
        in_specs=[vmem] * 4,
        out_specs=(hbm,) * 4,
        scratch_shapes=[dma((4,))],
        compiler_params=pltpu.CompilerParams(vmem_limit_bytes=1024 * 1024),
    )(*held)


def solution(mesh):
    n, tp = mesh.shape["kv"], mesh.shape["tp"]
    placed = (P("kv", "tp"),) * 5 + (P(),)
    return jax.shard_map(
        functools.partial(body, n, tp),
        mesh=mesh,
        in_specs=placed,
        out_specs=(P("kv", "tp"),) * 4,
        check_vma=False,
    )
```
